32 devices in a mesh: grp: 2 (over y), ep: 4 (over z), tp: 4 (over x, core).
Axes of the slice: x: 2, y: 2, z: 4, core: 2. Of those that a mesh axis runs over, the one named last changes fastest.
Arguments:
- query_first: bfloat16 [3072, 512], P(('grp', 'ep'), 'tp'), parts along dimension 0, may hold values from -32 to 32
- query_second: bfloat16 [3072, 512], P(('grp', 'ep'), 'tp'), parts along dimension 0, may hold values from -32 to 32
- key_first: bfloat16 [3072, 512], P(('grp', 'ep'), 'tp'), parts along dimension 0, may hold values from -32 to 32
- key_second: bfloat16 [3072, 512], P(('grp', 'ep'), 'tp'), parts along dimension 0, may hold values from -32 to 32
- values: bfloat16 [3072, 1024], P(('grp', 'ep'), 'tp'), parts along dimension 0, may hold values from -6 to 6
- lambda_head: float32 [8], P('tp'), may hold values from 0.3 to 0.8
- head_gain: float32 [128], replicated, may hold values from 0.1 to 1.9
- out_weight: bfloat16 [1024, 2048], replicated, may hold values from -0.1875 to 0.1875
- tokens: bfloat16 [4096, 2048], P(('grp', 'ep', 'tp')), parts along dimension 0, may hold values from -6 to 6
- norm_gain: float32 [2048], replicated, may hold values from 0.1 to 1.9
- expert_ids: int32 [4096, 2], P(('grp', 'ep', 'tp')), parts along dimension 0, may hold values from 0 to 3, all different within a row; in each aligned block of 128 rows (0 to 127, 128 to 255, ...) at most 96 rows name the same one
- expert_weights: float32 [4096, 2], P(('grp', 'ep', 'tp')), parts along dimension 0, may hold values from 0.2 to 1
- expert_gate: bfloat16 [4, 2048, 1024], P('ep', None, 'tp'), may hold values from -0.125 to 0.125
- expert_up: bfloat16 [4, 2048, 1024], P('ep', None, 'tp'), may hold values from -0.125 to 0.125
- expert_down: bfloat16 [4, 1024, 2048], P('ep', 'tp'), may hold values from -0.1875 to 0.1875
- shared_gate: bfloat16 [2048, 512], P(None, 'tp'), may hold values from -0.125 to 0.125
- shared_up: bfloat16 [2048, 512], P(None, 'tp'), may hold values from -0.125 to 0.125
- shared_down: bfloat16 [512, 2048], P('tp'), may hold values from -0.25 to 0.25
Outputs:
- mixed: bfloat16 [3072, 2048], P(('grp', 'ep', 'tp')), parts along dimension 0
- expert_out: bfloat16 [4096, 2048], P(('grp', 'ep', 'tp')), parts along dimension 0
The draws below stay inside these ranges and needn't reach their ends.
There are 2 independent parts, one for each index of `grp`. The reference program is written for one: setup_inputs(seed, part) draws one part's arguments, and reference() takes and returns one part's arrays. A program takes and returns all parts, laid end to end along the dimension named above; an argument that names none is the same for every part. Nothing has to cross between parts.
Inputs may be any that keep to these rules, and one draw needn't show every extreme that they name: `expert_ids`: in the rows of one device (aligned blocks of 128 rows) no expert is named by more than 96 rows, and in every draw some expert is named by exactly 96 rows of some block; each row names 2 different experts.
All inputs are finite; a program needn't handle non-finite values.
Results may differ from the reference program's by a relative error of at most 0.012.
Values may be sent and summed in bfloat16 or wider, within the bound.
A program may use at most 128 MiB of HBM per device.

```python
import math
import jax
import jax.numpy as jnp
import numpy as np
from jax import lax

D = 2048
HEADS = 8
HEAD = 64
VDIM = 128
FF = 1024
SHARED = 512
TOPK = 2
ROW_DEV = 128
TOKENS_A = 1536
TOKENS_E = 2048
EXPERTS = 4
CAP = 96
N_TP = 4


def drawn_pair(key, which):
    base = jax.random.fold_in(key, 4100 + which)
    key_query, key_keys = jax.random.split(base, 2)
    shape = (TOKENS_A, HEADS * HEAD)
    queries = 1.3 * jax.random.truncated_normal(key_query, -3.8, 3.8, shape, jnp.float32)
    keys = 1.3 * jax.random.truncated_normal(key_keys, -3.8, 3.8, shape, jnp.float32)
    return (queries.astype(jnp.bfloat16), keys.astype(jnp.bfloat16))


def draw_query_first(key, part):
    return drawn_pair(key, 0)[0]


def draw_key_first(key, part):
    return drawn_pair(key, 0)[1]


def draw_query_second(key, part):
    return drawn_pair(key, 1)[0]


def draw_key_second(key, part):
    return drawn_pair(key, 1)[1]


def steps_of(key, dims, cuts, smallest, largest):
    level = 1.0
    for dim, parts in cuts:
        heights = jax.random.uniform(jax.random.fold_in(jax.random.fold_in(key, 6), dim), (parts,), jnp.float32, smallest / len(cuts), largest / len(cuts))
        level = level * jnp.repeat(jnp.exp(heights), dims[dim] // parts).reshape((-1,) + (1,) * (len(dims) - 1 - dim))
    return level


def deal_out(key, own, number, rows, number_of, top, bound, slope):
    sequence = jax.random.permutation(key, number_of)
    heavy_load, ordinary = portions_of(number_of, rows * top, bound, slope, True), portions_of(number_of, rows * top, bound, slope, False)
    places = jnp.arange(number_of)

    def named(lengths, turn):
        used = int((lengths > 0).sum())
        fixed = max(1, used // 4)
        shifted = fixed + (places - fixed + turn * (used - fixed)) % max(1, number_of - fixed)
        return jnp.zeros((number_of,), jnp.int32).at[sequence[jnp.where(places < fixed, places, shifted)]].set(jnp.asarray(lengths, jnp.int32))

    lengths = jnp.where(number % 4 == 0, named(heavy_load, number // 4), named(ordinary, number - number // 4 - 1))
    mixed = jax.random.permutation(jax.random.fold_in(own, 3), number_of)
    donor, receiver = mixed[0:number_of // 2 * 2:2], mixed[1:number_of // 2 * 2:2]
    slack = jnp.minimum(lengths[donor] - 1, bound - lengths[receiver]) // 2
    slack = jnp.where((donor == sequence[0]) | (receiver == sequence[0]) | (lengths[receiver] == 0), 0, jnp.maximum(slack, 0))
    shifted = jax.random.randint(jax.random.fold_in(own, 4), (number_of // 2,), 0, 1 << 20) % (slack + 1)
    lengths = lengths.at[donor].add(-shifted).at[receiver].add(shifted)
    items = jnp.searchsorted(jnp.cumsum(lengths), jnp.arange(rows * top), side="right").astype(jnp.int32)
    grid = items.reshape(top, rows).T
    grid = grid[jax.random.permutation(jax.random.fold_in(own, 1), rows)]
    turn = jax.random.randint(jax.random.fold_in(own, 2), (rows, 1), 0, top)
    return jnp.take_along_axis(grid, (jnp.arange(top)[None, :] + turn) % top, axis=1)


def portions_of(number_of, total, most, skew, full):
    portions = [(1 << 20) // math.isqrt(rank ** skew) + 1 for rank in range(1, number_of + 1)]
    largest = most if full else min(most, max(-(-total // number_of), total * portions[0] // sum(portions)))
    least = 1 if total - largest >= number_of - 1 else 0
    counts, rest = [largest] + [least] * (number_of - 1), total - largest - least * (number_of - 1)
    while rest > 0:
        movable = [i for i in range(1, number_of) if counts[i] < largest] or [i for i in range(1, number_of) if counts[i] < most]
        whole, budget = sum([portions[i] for i in movable]), rest
        for i in movable:
            addition = min(most - counts[i], max(1, budget * portions[i] // whole), rest)
            counts[i] = counts[i] + addition
            rest = rest - addition
    return np.array(counts)


def centred(stream_key, shape, scale, limit, shards=(), held_as=jnp.bfloat16):
    drawn = jax.random.normal(stream_key, shape, jnp.float32) * scale
    if len(shards) > 0:
        drawn = steps_of(stream_key, shape, shards, -0.22, 0.18) * drawn
    return jnp.clip(drawn, min=-limit, max=limit).astype(held_as)


def setup_inputs(seed: int = 0, part: int = 0) -> dict:
    streams_of = jax.random.split(jax.random.key(seed), 19)
    part_keys = jax.random.split(jax.random.fold_in(streams_of[18], part), 19)
    query_first = draw_query_first(jax.random.fold_in(jax.random.fold_in(streams_of[18], part), 71), part)
    query_second = draw_query_second(jax.random.fold_in(jax.random.fold_in(streams_of[18], part), 71), part)
    key_first = draw_key_first(jax.random.fold_in(jax.random.fold_in(streams_of[18], part), 71), part)
    key_second = draw_key_second(jax.random.fold_in(jax.random.fold_in(streams_of[18], part), 71), part)
    values = centred(part_keys[4], (TOKENS_A, HEADS * VDIM), 1.0, 6.0, ((0, 4), (1, 4)))
    lambda_head = jnp.clip(0.3 + 0.5 * jax.random.uniform(streams_of[5], (HEADS,), jnp.float32) ** steps_of(streams_of[5], (HEADS,), ((0, 4),), -0.2, 0.2), 0.3, 0.8)
    head_gain = jnp.clip(1.0 + 0.18 * jax.random.normal(streams_of[6], (VDIM,), jnp.float32), 0.1, 1.9)
    out_weight = centred(streams_of[7], (HEADS * VDIM, D), (HEADS * VDIM) ** -0.5, 0.1875)
    tokens = centred(part_keys[8], (TOKENS_E, D), 1.0, 6.0, ((0, 16),))
    norm_gain = jnp.clip(1.0 + 0.18 * jax.random.normal(streams_of[9], (D,), jnp.float32), 0.1, 1.9)
    expert_ids_keys = jax.random.split(jax.random.fold_in(part_keys[10], 1), TOKENS_E // ROW_DEV)
    expert_ids_turns = jax.random.permutation(jax.random.fold_in(part_keys[10], 3), TOKENS_E // ROW_DEV)
    expert_ids = jax.vmap(lambda own, number: deal_out(jax.random.fold_in(part_keys[10], 2), own, number, ROW_DEV, EXPERTS, TOPK, CAP, 1))(expert_ids_keys, expert_ids_turns).reshape((TOKENS_E, TOPK))
    expert_weights = jnp.clip(0.2 + 0.8 * jax.random.uniform(part_keys[11], (TOKENS_E, TOPK), jnp.float32) ** steps_of(part_keys[11], (TOKENS_E, TOPK), ((0, 16),), -0.2, 0.2), 0.2, 1.0)
    expert_gate = centred(streams_of[12], (EXPERTS, D, FF), D ** -0.5, 0.125, ((0, 4), (2, 4)))
    expert_up = centred(streams_of[13], (EXPERTS, D, FF), D ** -0.5, 0.125, ((0, 4), (2, 4)))
    expert_down = centred(streams_of[14], (EXPERTS, FF, D), FF ** -0.5, 0.1875, ((0, 4), (1, 4)))
    shared_gate = centred(streams_of[15], (D, SHARED), D ** -0.5, 0.125, ((1, 4),))
    shared_up = centred(streams_of[16], (D, SHARED), D ** -0.5, 0.125, ((1, 4),))
    shared_down = centred(streams_of[17], (SHARED, D), SHARED ** -0.5, 0.25, ((0, 4),))
    return {"query_first": query_first, "query_second": query_second, "key_first": key_first, "key_second": key_second, "values": values, "lambda_head": lambda_head, "head_gain": head_gain, "out_weight": out_weight, "tokens": tokens, "norm_gain": norm_gain, "expert_ids": expert_ids, "expert_weights": expert_weights, "expert_gate": expert_gate, "expert_up": expert_up, "expert_down": expert_down, "shared_gate": shared_gate, "shared_up": shared_up, "shared_down": shared_down}


epsilon = 1e-06

def reference(query_first, query_second, key_first, key_second, values, lambda_head, head_gain, out_weight, tokens, norm_gain, expert_ids, expert_weights, expert_gate, expert_up, expert_down, shared_gate, shared_up, shared_down):
    score_scale = HEAD ** (-0.5)
    key_one = key_first.astype(jnp.float32).reshape(TOKENS_A, HEADS, HEAD)
    key_two = key_second.astype(jnp.float32).reshape(TOKENS_A, HEADS, HEAD)
    value_all = values.astype(jnp.float32).reshape(TOKENS_A, HEADS, VDIM)
    query_rows = math.gcd(TOKENS_A, 256)

    def one_map(queries, keys):
        scores = jnp.einsum('qhd,khd->qhk', queries, keys) * score_scale
        row_peak = lax.optimization_barrier(jnp.max(scores, axis=-1, keepdims=True))
        exponent = jnp.exp(scores - row_peak)
        row_total = lax.optimization_barrier(jnp.sum(exponent, axis=-1))
        rounded = lax.optimization_barrier(exponent.astype(jnp.bfloat16)).astype(jnp.float32)
        return jnp.einsum('qhk,khe->qhe', rounded, value_all) / row_total[..., None]

    def query_block(query_pair):
        first_block, second_block = query_pair
        mixture = one_map(first_block, key_one) - lambda_head[None, :, None] * one_map(second_block, key_two)
        normed_heads = mixture * lax.rsqrt(lax.optimization_barrier(jnp.mean(mixture * mixture, axis=-1, keepdims=True)) + epsilon) * head_gain
        return normed_heads.astype(jnp.bfloat16)
    query_one = query_first.astype(jnp.float32).reshape(TOKENS_A // query_rows, query_rows, HEADS, HEAD)
    query_two = query_second.astype(jnp.float32).reshape(TOKENS_A // query_rows, query_rows, HEADS, HEAD)
    head_rows = lax.map(query_block, (query_one, query_two)).reshape(TOKENS_A, HEADS * VDIM)
    mixed = jnp.dot(head_rows, out_weight, preferred_element_type=jnp.float32).astype(jnp.bfloat16)
    widened = tokens.astype(jnp.float32)
    normed = (widened * lax.rsqrt(lax.optimization_barrier(jnp.mean(widened * widened, axis=-1, keepdims=True)) + epsilon) * norm_gain).astype(jnp.bfloat16)
    block_count = TOKENS_E // ROW_DEV
    copies = ROW_DEV * TOPK
    chosen = expert_ids.reshape(block_count, copies)
    onehot = (chosen[:, :, None] == jnp.arange(EXPERTS, dtype=jnp.int32)[None, None, :]).astype(jnp.int32)
    rank_in_block = lax.optimization_barrier(jnp.sum(onehot * jnp.cumsum(onehot, axis=1), axis=-1)) - 1
    block_index = jnp.arange(block_count, dtype=jnp.int32)[:, None]
    slot_index = (chosen * (block_count * CAP) + block_index * CAP + rank_in_block).reshape(-1)
    token_index = (block_index * ROW_DEV + jnp.arange(copies, dtype=jnp.int32)[None, :] // TOPK).reshape(-1)
    slot_tokens = jnp.full((EXPERTS * block_count * CAP,), TOKENS_E, jnp.int32).at[slot_index].set(token_index)
    slot_tokens = slot_tokens.reshape(EXPERTS, block_count * CAP)
    slot_weights = jnp.zeros((EXPERTS * block_count * CAP,), jnp.float32).at[slot_index].set(expert_weights.reshape(-1))
    slot_weights = slot_weights.reshape(EXPERTS, block_count * CAP)
    padded = jnp.concatenate([normed, jnp.zeros((1, D), jnp.bfloat16)], axis=0)

    def expert_step(accum, inputs):
        index_rows, weight_rows, gate_matrix, up_matrix, down_matrix = inputs
        picked = padded[index_rows]
        gate_value = jnp.dot(picked, gate_matrix, preferred_element_type=jnp.float32)
        up_value = jnp.dot(picked, up_matrix, preferred_element_type=jnp.float32)
        hidden = (jax.nn.silu(gate_value) * up_value).astype(jnp.bfloat16)
        grouped = hidden.astype(jnp.float32).reshape(-1, N_TP, FF // N_TP)
        down_groups = down_matrix.astype(jnp.float32).reshape(N_TP, FF // N_TP, D)
        partial_value = jnp.einsum('mjf,jfd->jmd', grouped, down_groups)
        rounded = lax.optimization_barrier(partial_value.astype(jnp.bfloat16)).astype(jnp.float32)
        routed = lax.optimization_barrier(lax.optimization_barrier(jnp.sum(rounded, axis=0)).astype(jnp.bfloat16)).astype(jnp.float32)
        return (accum.at[index_rows].add(routed * weight_rows[:, None]), None)
    accum_start = jnp.zeros((TOKENS_E + 1, D), jnp.float32)
    routed_sum, unused = lax.scan(expert_step, accum_start, (slot_tokens, slot_weights, expert_gate, expert_up, expert_down))
    group_width = SHARED // N_TP
    shared_part = jnp.zeros((TOKENS_E, D), jnp.float32)
    for quarter in range(N_TP):
        columns = slice(quarter * group_width, (quarter + 1) * group_width)
        gate_value = jnp.dot(normed, shared_gate[:, columns], preferred_element_type=jnp.float32)
        up_value = jnp.dot(normed, shared_up[:, columns], preferred_element_type=jnp.float32)
        shared_hidden = (jax.nn.silu(gate_value) * up_value).astype(jnp.bfloat16)
        partial_value = jnp.dot(shared_hidden, shared_down[columns, :], preferred_element_type=jnp.float32)
        shared_part = shared_part + lax.optimization_barrier(partial_value.astype(jnp.bfloat16)).astype(jnp.float32)
    expert_out = (routed_sum[:TOKENS_E] + shared_part).astype(jnp.bfloat16)
    return (mixed, expert_out)
```

```python
import jax
import jax.numpy as jnp
from jax import lax
from jax.experimental import pallas as pl
from jax.experimental.pallas import tpu as pltpu
import functools
from jax.sharding import PartitionSpec as P

epsilon = 1e-06
block_limit = 1536


def key_block(total_rows, shard_rows):
    if total_rows <= block_limit or total_rows % shard_rows != 0:
        return total_rows
    best_rows = shard_rows
    for factor_rows in range(1, total_rows // shard_rows + 1):
        if total_rows % (factor_rows * shard_rows) == 0 and factor_rows * shard_rows <= block_limit:
            best_rows = factor_rows * shard_rows
    return best_rows


def softmax_update(states, scores, value_block):
    running_max, running_sum, accumulated = states
    new_max = jnp.maximum(running_max, jnp.max(scores, axis=-1))
    rescale = jnp.exp(running_max - new_max)
    weights = jnp.exp(scores - new_max[..., None])
    new_sum = running_sum * rescale + jnp.sum(weights, axis=-1)
    product = jnp.einsum(
        "qhk,khe->qhe",
        weights.astype(jnp.bfloat16),
        value_block,
        preferred_element_type=jnp.float32,
    )
    return (new_max, new_sum, accumulated * rescale[..., None] + product)


def shards(
    query_first,
    query_second,
    key_first,
    key_second,
    values,
    lambda_head,
    head_gain,
    out_weight,
    tokens,
    norm_gain,
    expert_ids,
    expert_weights,
    expert_gate,
    expert_up,
    expert_down,
    shared_gate,
    shared_up,
    shared_down,
):
    shard_rows, query_width = query_first.shape
    heads_here = lambda_head.shape[0]
    head_size = query_width // heads_here
    value_size = values.shape[1] // heads_here
    score_scale = head_size ** (-0.5)
    query_one = query_first.reshape(shard_rows, heads_here, head_size)
    query_two = query_second.reshape(shard_rows, heads_here, head_size)
    initial = (
        jnp.full((shard_rows, heads_here), -jnp.inf, jnp.float32),
        jnp.zeros((shard_rows, heads_here), jnp.float32),
        jnp.zeros((shard_rows, heads_here, value_size), jnp.float32),
    )
    carried = (initial, initial)
    key_one = lax.all_gather(key_first, "ep", axis=0, tiled=True)
    key_two = lax.all_gather(key_second, "ep", axis=0, tiled=True)
    value_piece = lax.all_gather(values, "ep", axis=0, tiled=True)
    total_rows = key_one.shape[0]
    block_rows = key_block(total_rows, shard_rows)
    block_count = total_rows // block_rows
    stacked = (
        key_one.reshape(block_count, block_rows, heads_here, head_size),
        key_two.reshape(block_count, block_rows, heads_here, head_size),
        value_piece.reshape(block_count, block_rows, heads_here, value_size),
    )

    def fold_step(states, blocks):
        first_state, second_state = states
        key_a, key_b, value_block = blocks
        scores_a = (
            jnp.einsum("qhd,khd->qhk", query_one, key_a, preferred_element_type=jnp.float32)
            * score_scale
        )
        scores_b = (
            jnp.einsum("qhd,khd->qhk", query_two, key_b, preferred_element_type=jnp.float32)
            * score_scale
        )
        return (
            (
                softmax_update(first_state, scores_a, value_block),
                softmax_update(second_state, scores_b, value_block),
            ),
            None,
        )

    carried, unused = lax.scan(fold_step, carried, stacked)
    first_state, second_state = carried
    first_out = first_state[2] / first_state[1][..., None]
    second_out = second_state[2] / second_state[1][..., None]
    mixture = first_out - lambda_head[None, :, None] * second_out
    normed_heads = (
        mixture
        * lax.rsqrt(jnp.mean(mixture * mixture, axis=-1, keepdims=True) + epsilon)
        * head_gain
    )
    head_local = normed_heads.astype(jnp.bfloat16).reshape(shard_rows, heads_here * value_size)
    position_heads = lax.all_to_all(head_local, "tp", split_axis=0, concat_axis=1, tiled=True)
    mixed = jnp.dot(position_heads, out_weight, preferred_element_type=jnp.float32).astype(
        jnp.bfloat16
    )
    row_count, model_width = tokens.shape
    top_count = expert_ids.shape[1]
    ep_count = lax.axis_size("ep")
    local_experts = expert_gate.shape[0]
    expert_count = local_experts * ep_count
    capacity = max(2, row_count * top_count * 3 // (2 * expert_count))
    routed_rows = expert_count * capacity
    owner_span = routed_rows + row_count
    widened = tokens.astype(jnp.float32)
    normed = (
        widened
        * lax.rsqrt(jnp.mean(widened * widened, axis=-1, keepdims=True) + epsilon)
        * norm_gain
    ).astype(jnp.bfloat16)
    flat_ids = expert_ids.reshape(-1)
    onehot = (flat_ids[:, None] == jnp.arange(expert_count, dtype=jnp.int32)[None, :]).astype(
        jnp.int32
    )
    ranks = jnp.sum(onehot * jnp.cumsum(onehot, axis=0), axis=1) - 1
    slot_index = flat_ids * capacity + ranks
    token_index = jnp.arange(flat_ids.shape[0], dtype=jnp.int32) // top_count
    filled = jnp.full((routed_rows,), row_count, jnp.int32).at[slot_index].set(token_index)
    padded = jnp.concatenate([normed, jnp.zeros((1, model_width), jnp.bfloat16)], axis=0)
    outgoing = padded[filled].reshape(1, ep_count, local_experts * capacity, model_width)
    arrived = lax.all_to_all(outgoing, "ep", split_axis=1, concat_axis=1, tiled=True)
    local_rows = jnp.concatenate(
        [arrived.reshape(1, routed_rows, model_width), normed[None]], axis=1
    )
    gathered = lax.all_gather(local_rows, "tp", axis=0, tiled=True)
    owners = owner_span * lax.axis_size("tp") // owner_span
    routed_in = gathered[:, :routed_rows].reshape(
        owners, ep_count, local_experts, capacity, model_width
    )
    gate_value = jnp.einsum(
        "osecd,edf->osecf", routed_in, expert_gate, preferred_element_type=jnp.float32
    )
    up_value = jnp.einsum(
        "osecd,edf->osecf", routed_in, expert_up, preferred_element_type=jnp.float32
    )
    hidden = (jax.nn.silu(gate_value) * up_value).astype(jnp.bfloat16)
    routed_out = jnp.einsum(
        "osecf,efd->osecd", hidden, expert_down, preferred_element_type=jnp.float32
    )
    routed_out = routed_out.reshape(owners, routed_rows, model_width)
    shared_in = gathered[:, routed_rows:]
    shared_gate_value = jnp.einsum(
        "ord,df->orf", shared_in, shared_gate, preferred_element_type=jnp.float32
    )
    shared_up_value = jnp.einsum(
        "ord,df->orf", shared_in, shared_up, preferred_element_type=jnp.float32
    )
    shared_hidden = (jax.nn.silu(shared_gate_value) * shared_up_value).astype(jnp.bfloat16)
    shared_out = jnp.einsum(
        "orf,fd->ord", shared_hidden, shared_down, preferred_element_type=jnp.float32
    )
    kept_rows = lax.psum_scatter(
        jnp.concatenate([routed_out, shared_out], axis=1)
        .reshape(owners * owner_span, model_width)
        .astype(jnp.bfloat16),
        "tp",
        scatter_dimension=0,
        tiled=True,
    ).astype(jnp.float32)
    routed_back = (
        kept_rows[:routed_rows]
        .astype(jnp.bfloat16)
        .reshape(ep_count, local_experts * capacity, model_width)
    )
    returned = lax.all_to_all(routed_back, "ep", split_axis=0, concat_axis=0, tiled=True).reshape(
        routed_rows, model_width
    )
    picked = returned[slot_index].reshape(row_count, top_count, model_width).astype(jnp.float32)
    combined = jnp.sum(picked * expert_weights[:, :, None], axis=1) + kept_rows[routed_rows:]
    expert_out = combined.astype(jnp.bfloat16)
    return (mixed, expert_out)


MESH = pl.DeviceIdType.MESH
BF = jnp.bfloat16
F32 = jnp.float32


def fused_fits(mesh):
    return mesh.shape["ep"] == 4 and mesh.shape["tp"] == 4


def fused_kernel(
    zn,
    tokens_ref,
    gain_ref,
    wloc_ref,
    qa_ref,
    qb_ref,
    ka_hbm,
    kb_hbm,
    v_hbm,
    lam_ref,
    hgain_ref,
    gate_hbm,
    up_hbm,
    down_hbm,
    sgate_hbm,
    sup_hbm,
    sdown_hbm,
    wo_hbm,
    mixed_ref,
    out_ref,
    gbuf,
    wbuf,
    kbuf,
    pbuf,
    abuf,
    bbuf,
    cbuf,
    hout,
    hbuf,
    gate,
    up,
    down,
    sgate,
    sup,
    sdown,
    wo,
    lsem,
    gsend,
    grecv,
    wsend,
    wrecv,
    ksend,
    krecv,
    asend,
    arecv,
    bsend,
    brecv,
    csend,
    crecv,
    hsend,
    hrecv,
):
    grp = lax.axis_index("grp")
    z = lax.axis_index("ep")
    t = lax.axis_index("tp")
    c = lax.rem(t, 2)
    x = lax.div(t, 2)
    partner = 2 * x + 1 - c
    peer = 2 * (1 - x) + c
    diag = 2 * (1 - x) + 1 - c
    tn = 4
    rows = tokens_ref.shape[0]
    width = tokens_ref.shape[1]
    arow = qa_ref.shape[0]
    kw = ka_hbm.shape[1]
    vw = v_hbm.shape[1]

    has_up = z < zn - 1
    has_dn = z > 0
    up_dev = (grp, jnp.minimum(z + 1, zn - 1), t)
    dn_dev = (grp, jnp.maximum(z - 1, 0), t)
    partner_dev = (grp, z, partner)
    peer_dev = (grp, z, peer)

    loads = [
        pltpu.make_async_copy(ka_hbm, kbuf.at[z, :, pl.ds(0, kw)], lsem.at[0]),
        pltpu.make_async_copy(kb_hbm, kbuf.at[z, :, pl.ds(kw, kw)], lsem.at[1]),
        pltpu.make_async_copy(v_hbm, kbuf.at[z, :, pl.ds(2 * kw, vw)], lsem.at[2]),
        pltpu.make_async_copy(gate_hbm.at[0], gate, lsem.at[3]),
        pltpu.make_async_copy(up_hbm.at[0], up, lsem.at[4]),
        pltpu.make_async_copy(down_hbm.at[0], down, lsem.at[5]),
        pltpu.make_async_copy(sgate_hbm, sgate, lsem.at[6]),
        pltpu.make_async_copy(sup_hbm, sup, lsem.at[7]),
        pltpu.make_async_copy(sdown_hbm, sdown, lsem.at[8]),
        pltpu.make_async_copy(wo_hbm, wo, lsem.at[9]),
    ]
    for load in loads:
        load.start()

    barrier = pltpu.get_barrier_semaphore()
    for other in (partner, peer, diag):
        pl.semaphore_signal(barrier, inc=1, device_id=(grp, z, other), device_id_type=MESH)

    @pl.when(has_up)
    def _():
        pl.semaphore_signal(barrier, inc=1, device_id=up_dev, device_id_type=MESH)

    @pl.when(has_dn)
    def _():
        pl.semaphore_signal(barrier, inc=1, device_id=dn_dev, device_id_type=MESH)

    own = z * tn + t
    wide = tokens_ref[...].astype(F32)
    scale = lax.rsqrt(jnp.mean(wide * wide, axis=-1, keepdims=True) + epsilon)
    gbuf[own] = (wide * scale * gain_ref[...]).astype(BF)
    wbuf[own] = wloc_ref[...]

    pl.semaphore_wait(barrier, 3 + jnp.where(has_up, 1, 0) + jnp.where(has_dn, 1, 0))

    def remote(src, dst, ssem, rsem, dev):
        return pltpu.make_async_remote_copy(
            src_ref=src, dst_ref=dst, send_sem=ssem, recv_sem=rsem, device_id=dev, device_id_type=MESH
        )

    def gcopies(slot, way, dev):
        return (
            remote(gbuf.at[slot], gbuf.at[slot], gsend.at[way, slot], grecv.at[slot], dev),
            remote(wbuf.at[slot], wbuf.at[slot], wsend.at[way, slot], wrecv.at[slot], dev),
        )

    def gstart(slot, way, dev):
        for one in gcopies(slot, way, dev):
            one.start()

    def gwait_recv(slot):
        for one in gcopies(slot, 0, partner_dev):
            one.wait_recv()

    def gwait_send(slot, way, dev):
        for one in gcopies(slot, way, dev):
            one.wait_send()

    def goes_up(k):
        return jnp.logical_and(has_up, k <= z)

    def goes_down(k):
        return jnp.logical_and(has_dn, k >= z)

    def order(j):
        low = jnp.minimum(z, zn - 1 - z)
        first = jnp.where(j < 2, 1 - j, j)
        near = jnp.where(low == 1, first, j)
        return jnp.where(z < 2, near, zn - 1 - near)

    def forward(k):
        slot = k * tn + t

        @pl.when(goes_up(k))
        def _():
            gstart(slot, 0, up_dev)

        @pl.when(goes_down(k))
        def _():
            gstart(slot, 1, dn_dev)

        gstart(slot, 2, peer_dev)
        gstart(slot, 3, partner_dev)

    forward(z)
    inner = jnp.minimum(z, zn - 1 - z)

    def kcopy(k, way, dev):
        return remote(kbuf.at[k], kbuf.at[k], ksend.at[way, k], krecv.at[k], dev)

    def kforward(k):
        @pl.when(goes_up(k))
        def _():
            kcopy(k, 0, up_dev).start()

        @pl.when(goes_down(k))
        def _():
            kcopy(k, 1, dn_dev).start()

    def acopy(k, xd):
        return remote(
            pbuf.at[k, 2 * xd + 1 - c], abuf.at[k, xd], asend.at[k, xd], arecv.at[k, xd], partner_dev
        )

    for load in loads[3:9]:
        load.wait()

    def silu_mul(g, u):
        return (g * (1.0 / (1.0 + jnp.exp(-g))) * u).astype(BF)

    def gather_step(j, carry):
        for i in range(1, 4):
            when = jnp.where(inner == 1, max(i - 2, 0), i - 1)

            @pl.when(j == when)
            def _():
                k = order(i)
                gwait_recv(k * tn + t)
                forward(k)
                if i == 3:
                    for load in loads[:3]:
                        load.wait()
                    kforward(z)

        k = order(j)
        gwait_recv(k * tn + peer)
        gstart(k * tn + peer, 3, partner_dev)
        gwait_recv(k * tn + partner)
        gwait_recv(k * tn + diag)
        rows_in = gbuf[pl.ds(k * tn, tn)].reshape(tn * rows, width)
        g = jnp.dot(rows_in, gate[...], preferred_element_type=F32)
        u = jnp.dot(rows_in, up[...], preferred_element_type=F32)
        hidden = silu_mul(g, u)
        pieces = []
        for s in range(tn):
            turned = wbuf[k * tn + s].T
            lane = lax.broadcasted_iota(jnp.int32, turned.shape, 1)
            pieces.append(jnp.sum(jnp.where(lane == z, turned, 0.0), axis=1, keepdims=True))
        weight = jnp.concatenate(pieces, axis=0)
        half = width // 2
        for h in range(2):
            cols = pl.ds(h * half, half)
            part = jnp.dot(hidden, down[:, h * half : (h + 1) * half], preferred_element_type=F32)
            pbuf[k, :, :, cols] = (part * weight).astype(BF).reshape(tn, rows, half)

        @pl.when(j == 0)
        def _():
            sg = jnp.dot(rows_in, sgate[...], preferred_element_type=F32)
            su = jnp.dot(rows_in, sup[...], preferred_element_type=F32)
            sh = silu_mul(sg, su)
            for h in range(2):
                cols = pl.ds(h * half, half)
                part = jnp.dot(sh, sdown[:, h * half : (h + 1) * half], preferred_element_type=F32)
                before = pbuf[k, :, :, cols].astype(F32)
                pbuf[k, :, :, cols] = (before + part.reshape(tn, rows, half)).astype(BF)

        for xd in range(2):
            acopy(k, xd).start()
        return carry

    lax.fori_loop(0, zn, gather_step, 0)

    def bcopy(k):
        return remote(pbuf.at[k, peer], bbuf.at[k], bsend.at[k], brecv.at[k], peer_dev)

    def pair_step(i, carry):
        k = order(zn - 1 - i)
        acopy(k, 0).wait_recv()
        acopy(k, 1).wait_recv()
        pbuf[k, peer] = (pbuf[k, peer].astype(F32) + abuf[k, 1 - x].astype(F32)).astype(BF)
        bcopy(k).start()
        pbuf[k, t] = (pbuf[k, t].astype(F32) + abuf[k, x].astype(F32)).astype(BF)
        return carry

    lax.fori_loop(0, zn, pair_step, 0)

    def key_step(j, carry):
        k = order(j)
        kcopy(k, 0, partner_dev).wait_recv()
        kforward(k)
        return carry

    lax.fori_loop(1, zn, key_step, 0)

    heads = vw // hgain_ref.shape[1]
    head = kw // heads
    vdim = vw // heads
    qrows = arow // 3

    def attend_step(i, carry):
        r = pl.multiple_of(i * qrows, qrows)
        for h in range(heads):
            lane = lax.broadcasted_iota(jnp.int32, (qrows, kw), 1)
            mine = jnp.logical_and(lane >= h * head, lane < (h + 1) * head)
            outs = []
            for m, q_ref in enumerate((qa_ref, qb_ref)):
                q = jnp.where(mine, q_ref[pl.ds(r, qrows), :], jnp.zeros((), BF))
                keys = kbuf[:, :, m * kw : (m + 1) * kw].reshape(zn * arow, kw)
                s = lax.dot_general(q, keys, (((1,), (1,)), ((), ())), preferred_element_type=F32)
                s = s * (head ** -0.5)
                peak = jnp.max(s, axis=-1, keepdims=True)
                e = jnp.exp(s - peak)
                total = jnp.sum(e, axis=-1, keepdims=True)
                vals = kbuf[:, :, 2 * kw + h * vdim : 2 * kw + (h + 1) * vdim].reshape(zn * arow, vdim)
                o = jnp.dot(e.astype(BF), vals, preferred_element_type=F32)
                outs.append(o / total)
            mix = outs[0] - lam_ref[0, h] * outs[1]
            norm = lax.rsqrt(jnp.mean(mix * mix, axis=-1, keepdims=True) + epsilon)
            hout[pl.ds(r, qrows), h * vdim : (h + 1) * vdim] = (mix * norm * hgain_ref[...]).astype(BF)
        return carry

    lax.fori_loop(0, 3, attend_step, 0)

    orow = arow // tn

    def hcopy(to):
        return remote(
            hout.at[pl.ds(pl.multiple_of(to * orow, 16), orow), :],
            hbuf.at[t],
            hsend.at[to],
            hrecv.at[t],
            (grp, z, to),
        )

    def hrecv_wait(src):
        remote(
            hout.at[pl.ds(0, orow), :], hbuf.at[src], hsend.at[src], hrecv.at[src], (grp, z, src)
        ).wait_recv()

    for other in (peer, diag, partner):
        hcopy(other).start()
    hbuf[t] = hout[pl.ds(pl.multiple_of(t * orow, 16), orow), :]

    def ccopy(k, way, dev):
        return remote(pbuf.at[k, t], cbuf.at[way, k], csend.at[k], crecv.at[way, k], dev)

    def line_step(i, carry):
        k = order(zn - 1 - i)
        bcopy(k).wait_recv()
        pbuf[k, t] = (pbuf[k, t].astype(F32) + bbuf[k].astype(F32)).astype(BF)

        @pl.when(k > z)
        def _():
            @pl.when(has_dn)
            def _():
                ccopy(k, 0, up_dev).wait_recv()
                pbuf[k, t] = (pbuf[k, t].astype(F32) + cbuf[0, k].astype(F32)).astype(BF)

            ccopy(k, 0, up_dev).start()

        @pl.when(k < z)
        def _():
            @pl.when(has_up)
            def _():
                ccopy(k, 1, dn_dev).wait_recv()
                pbuf[k, t] = (pbuf[k, t].astype(F32) + cbuf[1, k].astype(F32)).astype(BF)

            ccopy(k, 1, dn_dev).start()

        return carry

    lax.fori_loop(0, zn - 1, line_step, 0)

    for other in (partner, peer, diag):
        hrecv_wait(other)
    loads[9].wait()
    half = width // 2
    for h in range(2):
        acc = jnp.zeros((orow, half), F32)
        for s in range(tn):
            acc = acc + jnp.dot(
                hbuf[s], wo[s * vw : (s + 1) * vw, h * half : (h + 1) * half], preferred_element_type=F32
            )
        mixed_ref[:, h * half : (h + 1) * half] = acc.astype(BF)

    bcopy(z).wait_recv()
    pbuf[z, t] = (pbuf[z, t].astype(F32) + bbuf[z].astype(F32)).astype(BF)

    @pl.when(has_dn)
    def _():
        ccopy(z, 0, up_dev).wait_recv()
        pbuf[z, t] = (pbuf[z, t].astype(F32) + cbuf[0, z].astype(F32)).astype(BF)

    @pl.when(has_up)
    def _():
        ccopy(z, 1, dn_dev).wait_recv()
        pbuf[z, t] = (pbuf[z, t].astype(F32) + cbuf[1, z].astype(F32)).astype(BF)

    out_ref[...] = pbuf[z, t]

    def drain_step(k, carry):
        slot = k * tn + t

        @pl.when(goes_up(k))
        def _():
            gwait_send(slot, 0, up_dev)
            kcopy(k, 0, up_dev).wait_send()

        @pl.when(goes_down(k))
        def _():
            gwait_send(slot, 1, dn_dev)
            kcopy(k, 1, dn_dev).wait_send()

        gwait_send(slot, 2, peer_dev)
        gwait_send(slot, 3, partner_dev)
        gwait_send(k * tn + peer, 3, partner_dev)
        for xd in range(2):
            acopy(k, xd).wait_send()
        bcopy(k).wait_send()

        @pl.when(k != z)
        def _():
            ccopy(k, 0, up_dev).wait_send()

        return carry

    lax.fori_loop(0, zn, drain_step, 0)
    for other in (partner, peer, diag):
        hcopy(other).wait_send()


def fused_shards(
    zn,
    query_first,
    query_second,
    key_first,
    key_second,
    values,
    lambda_head,
    head_gain,
    out_weight,
    tokens,
    norm_gain,
    expert_ids,
    expert_weights,
    expert_gate,
    expert_up,
    expert_down,
    shared_gate,
    shared_up,
    shared_down,
):
    rows, width = tokens.shape
    arow, kw = key_first.shape
    vw = values.shape[1]
    tn = lax.axis_size("tp")
    pad = 8
    names = jnp.arange(pad, dtype=jnp.int32)[:, None]
    wloc = jnp.zeros((pad, rows), F32)
    for top in range(expert_ids.shape[1]):
        wloc = wloc + jnp.where(expert_ids[:, top][None, :] == names, expert_weights[:, top][None, :], 0.0)
    vmem = pl.BlockSpec(memory_space=pltpu.VMEM)
    smem = pl.BlockSpec(memory_space=pltpu.SMEM)
    hbm = pl.BlockSpec(memory_space=pltpu.HBM)
    dma = pltpu.SemaphoreType.DMA
    slots = zn * tn
    hidden = expert_gate.shape[2]
    shared = shared_gate.shape[1]
    mixed, expert_out = pl.pallas_call(
        functools.partial(fused_kernel, zn),
        out_shape=(
            jax.ShapeDtypeStruct((arow // tn, width), BF),
            jax.ShapeDtypeStruct((rows, width), BF),
        ),
        in_specs=[vmem, vmem, vmem, vmem, vmem, hbm, hbm, hbm, smem, vmem] + [hbm] * 7,
        out_specs=(vmem, vmem),
        scratch_shapes=[
            pltpu.VMEM((slots, rows, width), BF),
            pltpu.VMEM((slots, pad, rows), F32),
            pltpu.VMEM((zn, arow, 2 * kw + vw), BF),
            pltpu.VMEM((zn, tn, rows, width), BF),
            pltpu.VMEM((zn, 2, rows, width), BF),
            pltpu.VMEM((zn, rows, width), BF),
            pltpu.VMEM((2, zn, rows, width), BF),
            pltpu.VMEM((arow, vw), BF),
            pltpu.VMEM((tn, arow // tn, vw), BF),
            pltpu.VMEM((width, hidden), BF),
            pltpu.VMEM((width, hidden), BF),
            pltpu.VMEM((hidden, width), BF),
            pltpu.VMEM((width, shared), BF),
            pltpu.VMEM((width, shared), BF),
            pltpu.VMEM((shared, width), BF),
            pltpu.VMEM(out_weight.shape, BF),
            dma((10,)),
            dma((4, slots)),
            dma((slots,)),
            dma((4, slots)),
            dma((slots,)),
            dma((2, zn)),
            dma((zn,)),
            dma((zn, 2)),
            dma((zn, 2)),
            dma((zn,)),
            dma((zn,)),
            dma((zn,)),
            dma((2, zn)),
            dma((tn,)),
            dma((tn,)),
        ],
        compiler_params=pltpu.CompilerParams(
            collective_id=0, has_side_effects=True, vmem_limit_bytes=66000000
        ),
    )(
        tokens,
        norm_gain[None, :],
        wloc,
        query_first,
        query_second,
        key_first,
        key_second,
        values,
        lambda_head[None, :],
        head_gain[None, :],
        expert_gate,
        expert_up,
        expert_down,
        shared_gate,
        shared_up,
        shared_down,
        out_weight,
    )
    return mixed, expert_out


def solution(mesh):
    placed = (
        P(("grp", "ep"), "tp"),
        P(("grp", "ep"), "tp"),
        P(("grp", "ep"), "tp"),
        P(("grp", "ep"), "tp"),
        P(("grp", "ep"), "tp"),
        P("tp"),
        P(),
        P(),
        P(("grp", "ep", "tp"), None),
        P(),
        P(("grp", "ep", "tp"), None),
        P(("grp", "ep", "tp"), None),
        P("ep", None, "tp"),
        P("ep", None, "tp"),
        P("ep", "tp", None),
        P(None, "tp"),
        P(None, "tp"),
        P("tp", None),
    )
    body = functools.partial(fused_shards, mesh.shape["ep"]) if fused_fits(mesh) else shards
    return jax.shard_map(
        body,
        mesh=mesh,
        in_specs=placed,
        out_specs=(P(("grp", "ep", "tp"), None), P(("grp", "ep", "tp"), None)),
        check_vma=False,
    )
```

```python
import jax
import jax.numpy as jnp
from jax import lax
from jax.experimental import pallas as pl
from jax.experimental.pallas import tpu as pltpu
import functools
from jax.sharding import PartitionSpec as P

epsilon = 1e-06
block_limit = 1536


def key_block(total_rows, shard_rows):
    if total_rows <= block_limit or total_rows % shard_rows != 0:
        return total_rows
    best_rows = shard_rows
    for factor_rows in range(1, total_rows // shard_rows + 1):
        if total_rows % (factor_rows * shard_rows) == 0 and factor_rows * shard_rows <= block_limit:
            best_rows = factor_rows * shard_rows
    return best_rows


def softmax_update(states, scores, value_block):
    running_max, running_sum, accumulated = states
    new_max = jnp.maximum(running_max, jnp.max(scores, axis=-1))
    rescale = jnp.exp(running_max - new_max)
    weights = jnp.exp(scores - new_max[..., None])
    new_sum = running_sum * rescale + jnp.sum(weights, axis=-1)
    product = jnp.einsum(
        "qhk,khe->qhe",
        weights.astype(jnp.bfloat16),
        value_block,
        preferred_element_type=jnp.float32,
    )
    return (new_max, new_sum, accumulated * rescale[..., None] + product)


def shards(
    query_first,
    query_second,
    key_first,
    key_second,
    values,
    lambda_head,
    head_gain,
    out_weight,
    tokens,
    norm_gain,
    expert_ids,
    expert_weights,
    expert_gate,
    expert_up,
    expert_down,
    shared_gate,
    shared_up,
    shared_down,
):
    shard_rows, query_width = query_first.shape
    heads_here = lambda_head.shape[0]
    head_size = query_width // heads_here
    value_size = values.shape[1] // heads_here
    score_scale = head_size ** (-0.5)
    query_one = query_first.reshape(shard_rows, heads_here, head_size)
    query_two = query_second.reshape(shard_rows, heads_here, head_size)
    initial = (
        jnp.full((shard_rows, heads_here), -jnp.inf, jnp.float32),
        jnp.zeros((shard_rows, heads_here), jnp.float32),
        jnp.zeros((shard_rows, heads_here, value_size), jnp.float32),
    )
    carried = (initial, initial)
    key_one = lax.all_gather(key_first, "ep", axis=0, tiled=True)
    key_two = lax.all_gather(key_second, "ep", axis=0, tiled=True)
    value_piece = lax.all_gather(values, "ep", axis=0, tiled=True)
    total_rows = key_one.shape[0]
    block_rows = key_block(total_rows, shard_rows)
    block_count = total_rows // block_rows
    stacked = (
        key_one.reshape(block_count, block_rows, heads_here, head_size),
        key_two.reshape(block_count, block_rows, heads_here, head_size),
        value_piece.reshape(block_count, block_rows, heads_here, value_size),
    )

    def fold_step(states, blocks):
        first_state, second_state = states
        key_a, key_b, value_block = blocks
        scores_a = (
            jnp.einsum("qhd,khd->qhk", query_one, key_a, preferred_element_type=jnp.float32)
            * score_scale
        )
        scores_b = (
            jnp.einsum("qhd,khd->qhk", query_two, key_b, preferred_element_type=jnp.float32)
            * score_scale
        )
        return (
            (
                softmax_update(first_state, scores_a, value_block),
                softmax_update(second_state, scores_b, value_block),
            ),
            None,
        )

    carried, unused = lax.scan(fold_step, carried, stacked)
    first_state, second_state = carried
    first_out = first_state[2] / first_state[1][..., None]
    second_out = second_state[2] / second_state[1][..., None]
    mixture = first_out - lambda_head[None, :, None] * second_out
    normed_heads = (
        mixture
        * lax.rsqrt(jnp.mean(mixture * mixture, axis=-1, keepdims=True) + epsilon)
        * head_gain
    )
    head_local = normed_heads.astype(jnp.bfloat16).reshape(shard_rows, heads_here * value_size)
    position_heads = lax.all_to_all(head_local, "tp", split_axis=0, concat_axis=1, tiled=True)
    mixed = jnp.dot(position_heads, out_weight, preferred_element_type=jnp.float32).astype(
        jnp.bfloat16
    )
    row_count, model_width = tokens.shape
    top_count = expert_ids.shape[1]
    ep_count = lax.axis_size("ep")
    local_experts = expert_gate.shape[0]
    expert_count = local_experts * ep_count
    capacity = max(2, row_count * top_count * 3 // (2 * expert_count))
    routed_rows = expert_count * capacity
    owner_span = routed_rows + row_count
    widened = tokens.astype(jnp.float32)
    normed = (
        widened
        * lax.rsqrt(jnp.mean(widened * widened, axis=-1, keepdims=True) + epsilon)
        * norm_gain
    ).astype(jnp.bfloat16)
    flat_ids = expert_ids.reshape(-1)
    onehot = (flat_ids[:, None] == jnp.arange(expert_count, dtype=jnp.int32)[None, :]).astype(
        jnp.int32
    )
    ranks = jnp.sum(onehot * jnp.cumsum(onehot, axis=0), axis=1) - 1
    slot_index = flat_ids * capacity + ranks
    token_index = jnp.arange(flat_ids.shape[0], dtype=jnp.int32) // top_count
    filled = jnp.full((routed_rows,), row_count, jnp.int32).at[slot_index].set(token_index)
    padded = jnp.concatenate([normed, jnp.zeros((1, model_width), jnp.bfloat16)], axis=0)
    outgoing = padded[filled].reshape(1, ep_count, local_experts * capacity, model_width)
    arrived = lax.all_to_all(outgoing, "ep", split_axis=1, concat_axis=1, tiled=True)
    local_rows = jnp.concatenate(
        [arrived.reshape(1, routed_rows, model_width), normed[None]], axis=1
    )
    gathered = lax.all_gather(local_rows, "tp", axis=0, tiled=True)
    owners = owner_span * lax.axis_size("tp") // owner_span
    routed_in = gathered[:, :routed_rows].reshape(
        owners, ep_count, local_experts, capacity, model_width
    )
    gate_value = jnp.einsum(
        "osecd,edf->osecf", routed_in, expert_gate, preferred_element_type=jnp.float32
    )
    up_value = jnp.einsum(
        "osecd,edf->osecf", routed_in, expert_up, preferred_element_type=jnp.float32
    )
    hidden = (jax.nn.silu(gate_value) * up_value).astype(jnp.bfloat16)
    routed_out = jnp.einsum(
        "osecf,efd->osecd", hidden, expert_down, preferred_element_type=jnp.float32
    )
    routed_out = routed_out.reshape(owners, routed_rows, model_width)
    shared_in = gathered[:, routed_rows:]
    shared_gate_value = jnp.einsum(
        "ord,df->orf", shared_in, shared_gate, preferred_element_type=jnp.float32
    )
    shared_up_value = jnp.einsum(
        "ord,df->orf", shared_in, shared_up, preferred_element_type=jnp.float32
    )
    shared_hidden = (jax.nn.silu(shared_gate_value) * shared_up_value).astype(jnp.bfloat16)
    shared_out = jnp.einsum(
        "orf,fd->ord", shared_hidden, shared_down, preferred_element_type=jnp.float32
    )
    kept_rows = lax.psum_scatter(
        jnp.concatenate([routed_out, shared_out], axis=1)
        .reshape(owners * owner_span, model_width)
        .astype(jnp.bfloat16),
        "tp",
        scatter_dimension=0,
        tiled=True,
    ).astype(jnp.float32)
    routed_back = (
        kept_rows[:routed_rows]
        .astype(jnp.bfloat16)
        .reshape(ep_count, local_experts * capacity, model_width)
    )
    returned = lax.all_to_all(routed_back, "ep", split_axis=0, concat_axis=0, tiled=True).reshape(
        routed_rows, model_width
    )
    picked = returned[slot_index].reshape(row_count, top_count, model_width).astype(jnp.float32)
    combined = jnp.sum(picked * expert_weights[:, :, None], axis=1) + kept_rows[routed_rows:]
    expert_out = combined.astype(jnp.bfloat16)
    return (mixed, expert_out)


MESH = pl.DeviceIdType.MESH
BF = jnp.bfloat16
F32 = jnp.float32


def fused_fits(mesh):
    return mesh.shape["grp"] == 2 and mesh.shape["ep"] == 4 and mesh.shape["tp"] == 4


def fused_kernel(
    zn,
    tokens_ref,
    gain_ref,
    wloc_ref,
    qa_ref,
    qb_ref,
    ka_hbm,
    kb_hbm,
    v_hbm,
    lam_ref,
    hgain_ref,
    gate_hbm,
    up_hbm,
    down_hbm,
    sgate_hbm,
    sup_hbm,
    sdown_hbm,
    wo_hbm,
    mixed_ref,
    out_ref,
    gbuf,
    wbuf,
    kbuf,
    pbuf,
    abuf,
    cbuf,
    hout,
    hbuf,
    gate,
    up,
    down,
    sgate,
    sup,
    sdown,
    wo,
    lsem,
    gsend,
    grecv,
    wsend,
    wrecv,
    ksend,
    krecv,
    asend,
    arecv,
    xsend,
    xrecv,
    ysend,
    yrecv,
    csend,
    crecv,
    hsend,
    hrecv,
):
    grp = lax.axis_index("grp")
    z = lax.axis_index("ep")
    t = lax.axis_index("tp")
    c = lax.rem(t, 2)
    x = lax.div(t, 2)
    partner = 2 * x + 1 - c
    peer = 2 * (1 - x) + c
    diag = 2 * (1 - x) + 1 - c
    tn = 4
    rows = tokens_ref.shape[0]
    width = tokens_ref.shape[1]
    arow = qa_ref.shape[0]
    kw = ka_hbm.shape[1]
    vw = v_hbm.shape[1]

    has_up = z < zn - 1
    has_dn = z > 0
    up_dev = (grp, jnp.minimum(z + 1, zn - 1), t)
    dn_dev = (grp, jnp.maximum(z - 1, 0), t)
    partner_dev = (grp, z, partner)
    peer_dev = (grp, z, peer)
    twin_dev = (1 - grp, z, t)

    loads = [
        pltpu.make_async_copy(ka_hbm, kbuf.at[z, :, pl.ds(0, kw)], lsem.at[0]),
        pltpu.make_async_copy(kb_hbm, kbuf.at[z, :, pl.ds(kw, kw)], lsem.at[1]),
        pltpu.make_async_copy(v_hbm, kbuf.at[z, :, pl.ds(2 * kw, vw)], lsem.at[2]),
        pltpu.make_async_copy(gate_hbm.at[0], gate.at[0], lsem.at[3]),
        pltpu.make_async_copy(up_hbm.at[0], up.at[0], lsem.at[4]),
        pltpu.make_async_copy(down_hbm.at[0], down.at[0], lsem.at[5]),
        pltpu.make_async_copy(sgate_hbm, sgate.at[0], lsem.at[6]),
        pltpu.make_async_copy(sup_hbm, sup.at[0], lsem.at[7]),
        pltpu.make_async_copy(sdown_hbm, sdown.at[0], lsem.at[8]),
        pltpu.make_async_copy(wo_hbm, wo, lsem.at[9]),
    ]
    for load in loads[3:] + loads[:3]:
        load.start()

    barrier = pltpu.get_barrier_semaphore()
    for other in (partner, peer, diag):
        pl.semaphore_signal(barrier, inc=1, device_id=(grp, z, other), device_id_type=MESH)
    pl.semaphore_signal(barrier, inc=1, device_id=twin_dev, device_id_type=MESH)

    @pl.when(has_up)
    def _():
        pl.semaphore_signal(barrier, inc=1, device_id=up_dev, device_id_type=MESH)

    @pl.when(has_dn)
    def _():
        pl.semaphore_signal(barrier, inc=1, device_id=dn_dev, device_id_type=MESH)

    own = 2 * z + c
    wide = tokens_ref[...].astype(F32)
    scale = lax.rsqrt(jnp.mean(wide * wide, axis=-1, keepdims=True) + epsilon)
    gbuf[own] = (wide * scale * gain_ref[...]).astype(BF)
    wbuf[own] = wloc_ref[...]

    pl.semaphore_wait(barrier, 4 + jnp.where(has_up, 1, 0) + jnp.where(has_dn, 1, 0))

    def remote(src, dst, ssem, rsem, dev):
        return pltpu.make_async_remote_copy(
            src_ref=src, dst_ref=dst, send_sem=ssem, recv_sem=rsem, device_id=dev, device_id_type=MESH
        )

    def gcopies(slot, way, dev):
        return (
            remote(gbuf.at[slot], gbuf.at[slot], gsend.at[way, slot], grecv.at[slot], dev),
            remote(wbuf.at[slot], wbuf.at[slot], wsend.at[way, slot], wrecv.at[slot], dev),
        )

    def gstart(slot, way, dev):
        for one in gcopies(slot, way, dev):
            one.start()

    def gwait_recv(slot):
        for one in gcopies(slot, 0, partner_dev):
            one.wait_recv()

    def gwait_send(slot, way, dev):
        for one in gcopies(slot, way, dev):
            one.wait_send()

    def goes_up(k):
        return jnp.logical_and(has_up, k <= z)

    def goes_down(k):
        return jnp.logical_and(has_dn, k >= z)

    def order(j):
        low = jnp.minimum(z, zn - 1 - z)
        first = jnp.where(j < 2, 1 - j, j)
        near = jnp.where(low == 1, first, j)
        return jnp.where(z < 2, near, zn - 1 - near)

    def forward(k):
        slot = 2 * k + c

        @pl.when(goes_up(k))
        def _():
            gstart(slot, 0, up_dev)

        @pl.when(goes_down(k))
        def _():
            gstart(slot, 1, dn_dev)

        gstart(slot, 2, partner_dev)

    forward(z)
    inner = jnp.minimum(z, zn - 1 - z)

    def kcopy(k, way, dev):
        return remote(kbuf.at[k], kbuf.at[k], ksend.at[way, k], krecv.at[k], dev)

    def kforward(k):
        @pl.when(goes_up(k))
        def _():
            kcopy(k, 0, up_dev).start()

        @pl.when(goes_down(k))
        def _():
            kcopy(k, 1, dn_dev).start()

    def acopy(k):
        return remote(pbuf.at[k, 1 - c], abuf.at[k], asend.at[k], arecv.at[k], partner_dev)

    def cuts(buf, parts):
        size = buf.shape[1] // (2 * parts)
        return [(buf, (grp * parts + q) * size, (parts - grp * parts + q) * size, size) for q in range(parts)]

    pieces = cuts(gate, 2) + cuts(up, 2) + cuts(down, 2) + cuts(sgate, 1) + cuts(sup, 1) + cuts(sdown, 1)

    def xcopy(p):
        buf, mine, _, size = pieces[p]
        span = pl.ds(pl.multiple_of(mine, 16), size)
        return remote(buf.at[0, span, :], buf.at[1, span, :], xsend.at[p], xrecv.at[p], peer_dev)

    def ycopy(p):
        buf, mine, _, size = pieces[p]
        span = pl.ds(pl.multiple_of(mine, 16), size)
        return remote(buf.at[1, span, :], buf.at[1, span, :], ysend.at[p], yrecv.at[p], twin_dev)

    def ycopy_in(p):
        buf, _, theirs, size = pieces[p]
        span = pl.ds(pl.multiple_of(theirs, 16), size)
        return remote(buf.at[1, span, :], buf.at[1, span, :], ysend.at[p], yrecv.at[p], twin_dev)

    for p in range(len(pieces)):
        if p % 2 == 0 and p < 6:
            loads[3 + p // 2].wait()
        if p >= 6:
            loads[p].wait()
        xcopy(p).start()
    for load in loads[:3]:
        load.wait()

    @pl.when(inner == 0)
    def _():
        kforward(z)

    def silu_mul(g, u):
        return (g * (1.0 / (1.0 + jnp.exp(-g))) * u).astype(BF)

    def expert_part(k, side, shared):
        rows_in = gbuf[pl.ds(2 * k, 2)].reshape(2 * rows, width)
        g = jnp.dot(rows_in, gate[side], preferred_element_type=F32)
        u = jnp.dot(rows_in, up[side], preferred_element_type=F32)
        hidden = silu_mul(g, u)
        columns = []
        for s in range(2):
            turned = wbuf[2 * k + s].T
            lane = lax.broadcasted_iota(jnp.int32, turned.shape, 1)
            columns.append(jnp.sum(jnp.where(lane == z, turned, 0.0), axis=1, keepdims=True))
        weight = jnp.concatenate(columns, axis=0)
        half = width // 2
        for h in range(2):
            span = slice(h * half, (h + 1) * half)
            part = jnp.dot(hidden, down[side, :, span], preferred_element_type=F32) * weight
            part = part.reshape(2, rows, half)
            if side == 1:
                part = part + pbuf[k, :, :, span].astype(F32)
            pbuf[k, :, :, span] = part.astype(BF)

        @pl.when(shared)
        def _():
            if side == 1:
                for p in range(6, 9):
                    ycopy_in(p).wait_recv()
            sg = jnp.dot(rows_in, sgate[side], preferred_element_type=F32)
            su = jnp.dot(rows_in, sup[side], preferred_element_type=F32)
            sh = silu_mul(sg, su)
            for h in range(2):
                span = slice(h * half, (h + 1) * half)
                part = jnp.dot(sh, sdown[side, :, span], preferred_element_type=F32)
                before = pbuf[k, :, :, span].astype(F32)
                pbuf[k, :, :, span] = (before + part.reshape(2, rows, half)).astype(BF)

    def gather_step(j, carry):
        for jj, arriving in enumerate(((0, 1), (2, 3), (4, 5), (6, 7, 8))):

            @pl.when(j == jj)
            def _():
                for p in arriving:
                    xcopy(p).wait_recv()
                    ycopy(p).start()

        for i in range(1, 4):
            when = jnp.where(inner == 1, max(i - 2, 0), i - 1)

            @pl.when(j == when)
            def _():
                k = order(i)
                gwait_recv(2 * k + c)
                forward(k)
                if i == 3:

                    @pl.when(inner == 1)
                    def _():
                        kforward(z)

        k = order(j)
        gwait_recv(2 * k + 1 - c)
        expert_part(k, 0, j == 0)
        return carry

    lax.fori_loop(0, zn, gather_step, 0)

    def key_step(j, carry):
        k = order(j)
        kcopy(k, 0, partner_dev).wait_recv()
        kforward(k)
        return carry

    @pl.when(inner == 1)
    def _():
        lax.fori_loop(1, zn, key_step, 0)

    for p in range(6):
        ycopy_in(p).wait_recv()

    def ccopy(k, h, way, dev):
        span = pl.ds(h * (rows // 2), rows // 2)
        return remote(
            pbuf.at[k, c, span, :], cbuf.at[way, k, span, :], csend.at[k, h], crecv.at[way, k, h], dev
        )

    def pair_sum(k):
        acopy(k).wait_recv()
        for h in range(2):
            span = pl.ds(h * (rows // 2), rows // 2)
            pbuf[k, c, span, :] = (pbuf[k, c, span, :].astype(F32) + abuf[k, span, :].astype(F32)).astype(BF)

            @pl.when(jnp.logical_and(z == 0, k > z))
            def _():
                ccopy(k, h, 0, up_dev).start()

            @pl.when(jnp.logical_and(z == zn - 1, k < z))
            def _():
                ccopy(k, h, 1, dn_dev).start()

    def finish_step(i, carry):
        k = order(zn - 1 - i)
        expert_part(k, 1, i == zn - 1)
        acopy(k).start()

        @pl.when(i > 0)
        def _():
            pair_sum(order(zn - i))

        return carry

    lax.fori_loop(0, zn, finish_step, 0)
    pair_sum(z)

    @pl.when(inner == 0)
    def _():
        lax.fori_loop(1, zn, key_step, 0)

    heads = vw // hgain_ref.shape[1]
    head = kw // heads
    vdim = vw // heads
    qrows = arow // 3

    def attend_step(i, carry):
        r = pl.multiple_of(i * qrows, qrows)
        for h in range(heads):
            lane = lax.broadcasted_iota(jnp.int32, (qrows, kw), 1)
            mine = jnp.logical_and(lane >= h * head, lane < (h + 1) * head)
            outs = []
            for m, q_ref in enumerate((qa_ref, qb_ref)):
                q = jnp.where(mine, q_ref[pl.ds(r, qrows), :], jnp.zeros((), BF))
                keys = kbuf[:, :, m * kw : (m + 1) * kw].reshape(zn * arow, kw)
                s = lax.dot_general(q, keys, (((1,), (1,)), ((), ())), preferred_element_type=F32)
                s = s * (head ** -0.5)
                peak = jnp.max(s, axis=-1, keepdims=True)
                e = jnp.exp(s - peak)
                total = jnp.sum(e, axis=-1, keepdims=True)
                vals = kbuf[:, :, 2 * kw + h * vdim : 2 * kw + (h + 1) * vdim].reshape(zn * arow, vdim)
                o = jnp.dot(e.astype(BF), vals, preferred_element_type=F32)
                outs.append(o / total)
            mix = outs[0] - lam_ref[0, h] * outs[1]
            norm = lax.rsqrt(jnp.mean(mix * mix, axis=-1, keepdims=True) + epsilon)
            hout[pl.ds(r, qrows), h * vdim : (h + 1) * vdim] = (mix * norm * hgain_ref[...]).astype(BF)
        return carry

    lax.fori_loop(0, 3, attend_step, 0)

    orow = arow // tn

    def hcopy(to):
        return remote(
            hout.at[pl.ds(pl.multiple_of(to * orow, 16), orow), :],
            hbuf.at[t],
            hsend.at[to],
            hrecv.at[t],
            (grp, z, to),
        )

    def hrecv_wait(src):
        remote(
            hout.at[pl.ds(0, orow), :], hbuf.at[src], hsend.at[src], hrecv.at[src], (grp, z, src)
        ).wait_recv()

    for other in (peer, diag, partner):
        hcopy(other).start()
    hbuf[t] = hout[pl.ds(pl.multiple_of(t * orow, 16), orow), :]

    def line_step(i, carry):
        k = order(zn - 1 - i)
        for h in range(2):
            span = pl.ds(h * (rows // 2), rows // 2)

            @pl.when(jnp.logical_and(k > z, has_dn))
            def _():
                ccopy(k, h, 0, up_dev).wait_recv()
                pbuf[k, c, span, :] = (
                    pbuf[k, c, span, :].astype(F32) + cbuf[0, k, span, :].astype(F32)
                ).astype(BF)
                ccopy(k, h, 0, up_dev).start()

            @pl.when(jnp.logical_and(k < z, has_up))
            def _():
                ccopy(k, h, 1, dn_dev).wait_recv()
                pbuf[k, c, span, :] = (
                    pbuf[k, c, span, :].astype(F32) + cbuf[1, k, span, :].astype(F32)
                ).astype(BF)
                ccopy(k, h, 1, dn_dev).start()

        return carry

    lax.fori_loop(0, zn - 1, line_step, 0)

    for other in (partner, peer, diag):
        hrecv_wait(other)
    loads[9].wait()
    half = width // 2
    for h in range(2):
        acc = jnp.zeros((orow, half), F32)
        for s in range(tn):
            acc = acc + jnp.dot(
                hbuf[s], wo[s * vw : (s + 1) * vw, h * half : (h + 1) * half], preferred_element_type=F32
            )
        mixed_ref[:, h * half : (h + 1) * half] = acc.astype(BF)

    for h in range(2):
        span = pl.ds(h * (rows // 2), rows // 2)

        @pl.when(has_dn)
        def _():
            ccopy(z, h, 0, up_dev).wait_recv()
            pbuf[z, c, span, :] = (
                pbuf[z, c, span, :].astype(F32) + cbuf[0, z, span, :].astype(F32)
            ).astype(BF)

        @pl.when(has_up)
        def _():
            ccopy(z, h, 1, dn_dev).wait_recv()
            pbuf[z, c, span, :] = (
                pbuf[z, c, span, :].astype(F32) + cbuf[1, z, span, :].astype(F32)
            ).astype(BF)

    out_ref[...] = pbuf[z, c]

    def drain_step(k, carry):
        slot = 2 * k + c

        @pl.when(goes_up(k))
        def _():
            gwait_send(slot, 0, up_dev)
            kcopy(k, 0, up_dev).wait_send()

        @pl.when(goes_down(k))
        def _():
            gwait_send(slot, 1, dn_dev)
            kcopy(k, 1, dn_dev).wait_send()

        gwait_send(slot, 2, partner_dev)
        acopy(k).wait_send()

        @pl.when(k != z)
        def _():
            for h in range(2):
                ccopy(k, h, 0, up_dev).wait_send()

        return carry

    for p in range(len(pieces)):
        xcopy(p).wait_send()
        ycopy(p).wait_send()
    lax.fori_loop(0, zn, drain_step, 0)
    for other in (partner, peer, diag):
        hcopy(other).wait_send()


def fused_shards(
    zn,
    query_first,
    query_second,
    key_first,
    key_second,
    values,
    lambda_head,
    head_gain,
    out_weight,
    tokens,
    norm_gain,
    expert_ids,
    expert_weights,
    expert_gate,
    expert_up,
    expert_down,
    shared_gate,
    shared_up,
    shared_down,
):
    rows, width = tokens.shape
    arow, kw = key_first.shape
    vw = values.shape[1]
    tn = lax.axis_size("tp")
    pad = 8
    names = jnp.arange(pad, dtype=jnp.int32)[:, None]
    wloc = jnp.zeros((pad, rows), F32)
    for top in range(expert_ids.shape[1]):
        wloc = wloc + jnp.where(expert_ids[:, top][None, :] == names, expert_weights[:, top][None, :], 0.0)
    vmem = pl.BlockSpec(memory_space=pltpu.VMEM)
    smem = pl.BlockSpec(memory_space=pltpu.SMEM)
    hbm = pl.BlockSpec(memory_space=pltpu.HBM)
    dma = pltpu.SemaphoreType.DMA
    slots = zn * 2
    hidden = expert_gate.shape[2]
    shared = shared_gate.shape[1]
    mixed, expert_out = pl.pallas_call(
        functools.partial(fused_kernel, zn),
        out_shape=(
            jax.ShapeDtypeStruct((arow // tn, width), BF),
            jax.ShapeDtypeStruct((rows, width), BF),
        ),
        in_specs=[vmem, vmem, vmem, vmem, vmem, hbm, hbm, hbm, smem, vmem] + [hbm] * 7,
        out_specs=(vmem, vmem),
        scratch_shapes=[
            pltpu.VMEM((slots, rows, width), BF),
            pltpu.VMEM((slots, pad, rows), F32),
            pltpu.VMEM((zn, arow, 2 * kw + vw), BF),
            pltpu.VMEM((zn, 2, rows, width), BF),
            pltpu.VMEM((zn, rows, width), BF),
            pltpu.VMEM((2, zn, rows, width), BF),
            pltpu.VMEM((arow, vw), BF),
            pltpu.VMEM((tn, arow // tn, vw), BF),
            pltpu.VMEM((2, width, hidden), BF),
            pltpu.VMEM((2, width, hidden), BF),
            pltpu.VMEM((2, hidden, width), BF),
            pltpu.VMEM((2, width, shared), BF),
            pltpu.VMEM((2, width, shared), BF),
            pltpu.VMEM((2, shared, width), BF),
            pltpu.VMEM(out_weight.shape, BF),
            dma((10,)),
            dma((3, slots)),
            dma((slots,)),
            dma((3, slots)),
            dma((slots,)),
            dma((2, zn)),
            dma((zn,)),
            dma((zn,)),
            dma((zn,)),
            dma((9,)),
            dma((9,)),
            dma((9,)),
            dma((9,)),
            dma((zn, 2)),
            dma((2, zn, 2)),
            dma((tn,)),
            dma((tn,)),
        ],
        compiler_params=pltpu.CompilerParams(
            collective_id=0, has_side_effects=True, vmem_limit_bytes=66000000
        ),
    )(
        tokens,
        norm_gain[None, :],
        wloc,
        query_first,
        query_second,
        key_first,
        key_second,
        values,
        lambda_head[None, :],
        head_gain[None, :],
        expert_gate,
        expert_up,
        expert_down,
        shared_gate,
        shared_up,
        shared_down,
        out_weight,
    )
    return mixed, expert_out


def solution(mesh):
    placed = (
        P(("grp", "ep"), "tp"),
        P(("grp", "ep"), "tp"),
        P(("grp", "ep"), "tp"),
        P(("grp", "ep"), "tp"),
        P(("grp", "ep"), "tp"),
        P("tp"),
        P(),
        P(),
        P(("grp", "ep", "tp"), None),
        P(),
        P(("grp", "ep", "tp"), None),
        P(("grp", "ep", "tp"), None),
        P("ep", None, "tp"),
        P("ep", None, "tp"),
        P("ep", "tp", None),
        P(None, "tp"),
        P(None, "tp"),
        P("tp", None),
    )
    body = functools.partial(fused_shards, mesh.shape["ep"]) if fused_fits(mesh) else shards
    return jax.shard_map(
        body,
        mesh=mesh,
        in_specs=placed,
        out_specs=(P(("grp", "ep", "tp"), None), P(("grp", "ep", "tp"), None)),
        check_vma=False,
    )
```

```python
import jax
import jax.numpy as jnp
from jax import lax
from jax.experimental import pallas as pl
from jax.experimental.pallas import tpu as pltpu
import functools
from jax.sharding import PartitionSpec as P

epsilon = 1e-06
block_limit = 1536


def key_block(total_rows, shard_rows):
    if total_rows <= block_limit or total_rows % shard_rows != 0:
        return total_rows
    best_rows = shard_rows
    for factor_rows in range(1, total_rows // shard_rows + 1):
        if total_rows % (factor_rows * shard_rows) == 0 and factor_rows * shard_rows <= block_limit:
            best_rows = factor_rows * shard_rows
    return best_rows


def softmax_update(states, scores, value_block):
    running_max, running_sum, accumulated = states
    new_max = jnp.maximum(running_max, jnp.max(scores, axis=-1))
    rescale = jnp.exp(running_max - new_max)
    weights = jnp.exp(scores - new_max[..., None])
    new_sum = running_sum * rescale + jnp.sum(weights, axis=-1)
    product = jnp.einsum(
        "qhk,khe->qhe",
        weights.astype(jnp.bfloat16),
        value_block,
        preferred_element_type=jnp.float32,
    )
    return (new_max, new_sum, accumulated * rescale[..., None] + product)


def shards(
    query_first,
    query_second,
    key_first,
    key_second,
    values,
    lambda_head,
    head_gain,
    out_weight,
    tokens,
    norm_gain,
    expert_ids,
    expert_weights,
    expert_gate,
    expert_up,
    expert_down,
    shared_gate,
    shared_up,
    shared_down,
):
    shard_rows, query_width = query_first.shape
    heads_here = lambda_head.shape[0]
    head_size = query_width // heads_here
    value_size = values.shape[1] // heads_here
    score_scale = head_size ** (-0.5)
    query_one = query_first.reshape(shard_rows, heads_here, head_size)
    query_two = query_second.reshape(shard_rows, heads_here, head_size)
    initial = (
        jnp.full((shard_rows, heads_here), -jnp.inf, jnp.float32),
        jnp.zeros((shard_rows, heads_here), jnp.float32),
        jnp.zeros((shard_rows, heads_here, value_size), jnp.float32),
    )
    carried = (initial, initial)
    key_one = lax.all_gather(key_first, "ep", axis=0, tiled=True)
    key_two = lax.all_gather(key_second, "ep", axis=0, tiled=True)
    value_piece = lax.all_gather(values, "ep", axis=0, tiled=True)
    total_rows = key_one.shape[0]
    block_rows = key_block(total_rows, shard_rows)
    block_count = total_rows // block_rows
    stacked = (
        key_one.reshape(block_count, block_rows, heads_here, head_size),
        key_two.reshape(block_count, block_rows, heads_here, head_size),
        value_piece.reshape(block_count, block_rows, heads_here, value_size),
    )

    def fold_step(states, blocks):
        first_state, second_state = states
        key_a, key_b, value_block = blocks
        scores_a = (
            jnp.einsum("qhd,khd->qhk", query_one, key_a, preferred_element_type=jnp.float32)
            * score_scale
        )
        scores_b = (
            jnp.einsum("qhd,khd->qhk", query_two, key_b, preferred_element_type=jnp.float32)
            * score_scale
        )
        return (
            (
                softmax_update(first_state, scores_a, value_block),
                softmax_update(second_state, scores_b, value_block),
            ),
            None,
        )

    carried, unused = lax.scan(fold_step, carried, stacked)
    first_state, second_state = carried
    first_out = first_state[2] / first_state[1][..., None]
    second_out = second_state[2] / second_state[1][..., None]
    mixture = first_out - lambda_head[None, :, None] * second_out
    normed_heads = (
        mixture
        * lax.rsqrt(jnp.mean(mixture * mixture, axis=-1, keepdims=True) + epsilon)
        * head_gain
    )
    head_local = normed_heads.astype(jnp.bfloat16).reshape(shard_rows, heads_here * value_size)
    position_heads = lax.all_to_all(head_local, "tp", split_axis=0, concat_axis=1, tiled=True)
    mixed = jnp.dot(position_heads, out_weight, preferred_element_type=jnp.float32).astype(
        jnp.bfloat16
    )
    row_count, model_width = tokens.shape
    top_count = expert_ids.shape[1]
    ep_count = lax.axis_size("ep")
    local_experts = expert_gate.shape[0]
    expert_count = local_experts * ep_count
    capacity = max(2, row_count * top_count * 3 // (2 * expert_count))
    routed_rows = expert_count * capacity
    owner_span = routed_rows + row_count
    widened = tokens.astype(jnp.float32)
    normed = (
        widened
        * lax.rsqrt(jnp.mean(widened * widened, axis=-1, keepdims=True) + epsilon)
        * norm_gain
    ).astype(jnp.bfloat16)
    flat_ids = expert_ids.reshape(-1)
    onehot = (flat_ids[:, None] == jnp.arange(expert_count, dtype=jnp.int32)[None, :]).astype(
        jnp.int32
    )
    ranks = jnp.sum(onehot * jnp.cumsum(onehot, axis=0), axis=1) - 1
    slot_index = flat_ids * capacity + ranks
    token_index = jnp.arange(flat_ids.shape[0], dtype=jnp.int32) // top_count
    filled = jnp.full((routed_rows,), row_count, jnp.int32).at[slot_index].set(token_index)
    padded = jnp.concatenate([normed, jnp.zeros((1, model_width), jnp.bfloat16)], axis=0)
    outgoing = padded[filled].reshape(1, ep_count, local_experts * capacity, model_width)
    arrived = lax.all_to_all(outgoing, "ep", split_axis=1, concat_axis=1, tiled=True)
    local_rows = jnp.concatenate(
        [arrived.reshape(1, routed_rows, model_width), normed[None]], axis=1
    )
    gathered = lax.all_gather(local_rows, "tp", axis=0, tiled=True)
    owners = owner_span * lax.axis_size("tp") // owner_span
    routed_in = gathered[:, :routed_rows].reshape(
        owners, ep_count, local_experts, capacity, model_width
    )
    gate_value = jnp.einsum(
        "osecd,edf->osecf", routed_in, expert_gate, preferred_element_type=jnp.float32
    )
    up_value = jnp.einsum(
        "osecd,edf->osecf", routed_in, expert_up, preferred_element_type=jnp.float32
    )
    hidden = (jax.nn.silu(gate_value) * up_value).astype(jnp.bfloat16)
    routed_out = jnp.einsum(
        "osecf,efd->osecd", hidden, expert_down, preferred_element_type=jnp.float32
    )
    routed_out = routed_out.reshape(owners, routed_rows, model_width)
    shared_in = gathered[:, routed_rows:]
    shared_gate_value = jnp.einsum(
        "ord,df->orf", shared_in, shared_gate, preferred_element_type=jnp.float32
    )
    shared_up_value = jnp.einsum(
        "ord,df->orf", shared_in, shared_up, preferred_element_type=jnp.float32
    )
    shared_hidden = (jax.nn.silu(shared_gate_value) * shared_up_value).astype(jnp.bfloat16)
    shared_out = jnp.einsum(
        "orf,fd->ord", shared_hidden, shared_down, preferred_element_type=jnp.float32
    )
    kept_rows = lax.psum_scatter(
        jnp.concatenate([routed_out, shared_out], axis=1)
        .reshape(owners * owner_span, model_width)
        .astype(jnp.bfloat16),
        "tp",
        scatter_dimension=0,
        tiled=True,
    ).astype(jnp.float32)
    routed_back = (
        kept_rows[:routed_rows]
        .astype(jnp.bfloat16)
        .reshape(ep_count, local_experts * capacity, model_width)
    )
    returned = lax.all_to_all(routed_back, "ep", split_axis=0, concat_axis=0, tiled=True).reshape(
        routed_rows, model_width
    )
    picked = returned[slot_index].reshape(row_count, top_count, model_width).astype(jnp.float32)
    combined = jnp.sum(picked * expert_weights[:, :, None], axis=1) + kept_rows[routed_rows:]
    expert_out = combined.astype(jnp.bfloat16)
    return (mixed, expert_out)


MESH = pl.DeviceIdType.MESH
BF = jnp.bfloat16
F32 = jnp.float32


def fused_fits(mesh):
    return mesh.shape["grp"] == 2 and mesh.shape["ep"] == 4 and mesh.shape["tp"] == 4


def fused_kernel(
    zn,
    tokens_ref,
    gain_ref,
    wloc_ref,
    qa_ref,
    qb_ref,
    ka_hbm,
    kb_hbm,
    v_hbm,
    lam_ref,
    hgain_ref,
    gate_hbm,
    up_hbm,
    down_hbm,
    sgate_hbm,
    sup_hbm,
    sdown_hbm,
    wo_hbm,
    mixed_ref,
    out_ref,
    gbuf,
    wbuf,
    kbuf,
    pbuf,
    abuf,
    cbuf,
    hout,
    hbuf,
    gate,
    up,
    down,
    sgate,
    sup,
    sdown,
    wo,
    lsem,
    gsend,
    grecv,
    wsend,
    wrecv,
    ksend,
    krecv,
    asend,
    arecv,
    xsend,
    xrecv,
    ysend,
    yrecv,
    csend,
    crecv,
    hsend,
    hrecv,
):
    grp = lax.axis_index("grp")
    z = lax.axis_index("ep")
    t = lax.axis_index("tp")
    c = lax.rem(t, 2)
    x = lax.div(t, 2)
    partner = 2 * x + 1 - c
    peer = 2 * (1 - x) + c
    diag = 2 * (1 - x) + 1 - c
    tn = 4
    rows = tokens_ref.shape[0]
    width = tokens_ref.shape[1]
    arow = qa_ref.shape[0]
    kw = ka_hbm.shape[1]
    vw = v_hbm.shape[1]

    has_up = z < zn - 1
    has_dn = z > 0
    up_dev = (grp, jnp.minimum(z + 1, zn - 1), t)
    dn_dev = (grp, jnp.maximum(z - 1, 0), t)
    partner_dev = (grp, z, partner)
    peer_dev = (grp, z, peer)
    twin_dev = (1 - grp, z, t)

    loads = [
        pltpu.make_async_copy(ka_hbm, kbuf.at[z, :, pl.ds(0, kw)], lsem.at[0]),
        pltpu.make_async_copy(kb_hbm, kbuf.at[z, :, pl.ds(kw, kw)], lsem.at[1]),
        pltpu.make_async_copy(v_hbm, kbuf.at[z, :, pl.ds(2 * kw, vw)], lsem.at[2]),
        pltpu.make_async_copy(gate_hbm.at[0], gate.at[0], lsem.at[3]),
        pltpu.make_async_copy(up_hbm.at[0], up.at[0], lsem.at[4]),
        pltpu.make_async_copy(down_hbm.at[0], down.at[0], lsem.at[5]),
        pltpu.make_async_copy(sgate_hbm, sgate.at[0], lsem.at[6]),
        pltpu.make_async_copy(sup_hbm, sup.at[0], lsem.at[7]),
        pltpu.make_async_copy(sdown_hbm, sdown.at[0], lsem.at[8]),
        pltpu.make_async_copy(wo_hbm, wo, lsem.at[9]),
    ]
    for load in loads[3:] + loads[:3]:
        load.start()

    barrier = pltpu.get_barrier_semaphore()
    for other in (partner, peer, diag):
        pl.semaphore_signal(barrier, inc=1, device_id=(grp, z, other), device_id_type=MESH)
    pl.semaphore_signal(barrier, inc=1, device_id=twin_dev, device_id_type=MESH)

    @pl.when(has_up)
    def _():
        pl.semaphore_signal(barrier, inc=1, device_id=up_dev, device_id_type=MESH)

    @pl.when(has_dn)
    def _():
        pl.semaphore_signal(barrier, inc=1, device_id=dn_dev, device_id_type=MESH)

    own = 2 * z + c
    wide = tokens_ref[...].astype(F32)
    scale = lax.rsqrt(jnp.mean(wide * wide, axis=-1, keepdims=True) + epsilon)
    gbuf[own] = (wide * scale * gain_ref[...]).astype(BF)
    wbuf[own] = wloc_ref[...]

    pl.semaphore_wait(barrier, 4 + jnp.where(has_up, 1, 0) + jnp.where(has_dn, 1, 0))

    def remote(src, dst, ssem, rsem, dev):
        return pltpu.make_async_remote_copy(
            src_ref=src, dst_ref=dst, send_sem=ssem, recv_sem=rsem, device_id=dev, device_id_type=MESH
        )

    def gcopies(slot, way, dev):
        return (
            remote(gbuf.at[slot], gbuf.at[slot], gsend.at[way, slot], grecv.at[slot], dev),
            remote(wbuf.at[slot], wbuf.at[slot], wsend.at[way, slot], wrecv.at[slot], dev),
        )

    def gstart(slot, way, dev):
        for one in gcopies(slot, way, dev):
            one.start()

    def gwait_recv(slot):
        for one in gcopies(slot, 0, partner_dev):
            one.wait_recv()

    def gwait_send(slot, way, dev):
        for one in gcopies(slot, way, dev):
            one.wait_send()

    def goes_up(k):
        return jnp.logical_and(has_up, k <= z)

    def goes_down(k):
        return jnp.logical_and(has_dn, k >= z)

    def order(j):
        low = jnp.minimum(z, zn - 1 - z)
        first = jnp.where(j < 2, 1 - j, j)
        near = jnp.where(low == 1, first, j)
        return jnp.where(z < 2, near, zn - 1 - near)

    def forward(k):
        slot = 2 * k + c

        @pl.when(goes_up(k))
        def _():
            gstart(slot, 0, up_dev)

        @pl.when(goes_down(k))
        def _():
            gstart(slot, 1, dn_dev)

        gstart(slot, 2, partner_dev)

    forward(z)
    inner = jnp.minimum(z, zn - 1 - z)

    def kcopy(k, way, dev):
        return remote(kbuf.at[k], kbuf.at[k], ksend.at[way, k], krecv.at[k], dev)

    def kforward(k):
        @pl.when(goes_up(k))
        def _():
            kcopy(k, 0, up_dev).start()

        @pl.when(goes_down(k))
        def _():
            kcopy(k, 1, dn_dev).start()

    def acopy(k):
        return remote(pbuf.at[k, 1 - c], abuf.at[k], asend.at[k], arecv.at[k], partner_dev)

    def cuts(buf, parts):
        size = buf.shape[1] // (2 * parts)
        return [(buf, (grp * parts + q) * size, (parts - grp * parts + q) * size, size) for q in range(parts)]

    pieces = cuts(gate, 2) + cuts(up, 2) + cuts(down, 4) + cuts(sgate, 1) + cuts(sup, 1) + cuts(sdown, 1)

    def xcopy(p):
        buf, mine, _, size = pieces[p]
        span = pl.ds(pl.multiple_of(mine, 16), size)
        return remote(buf.at[0, span, :], buf.at[1, span, :], xsend.at[p], xrecv.at[p], peer_dev)

    def ycopy(p):
        buf, mine, _, size = pieces[p]
        span = pl.ds(pl.multiple_of(mine, 16), size)
        return remote(buf.at[1, span, :], buf.at[1, span, :], ysend.at[p], yrecv.at[p], twin_dev)

    def ycopy_in(p):
        buf, _, theirs, size = pieces[p]
        span = pl.ds(pl.multiple_of(theirs, 16), size)
        return remote(buf.at[1, span, :], buf.at[1, span, :], ysend.at[p], yrecv.at[p], twin_dev)

    for p in range(len(pieces)):
        if p in (0, 2, 4):
            loads[3 + p // 2].wait()
        if p >= 8:
            loads[p - 2].wait()
        xcopy(p).start()
    for load in loads[:3]:
        load.wait()

    @pl.when(inner == 0)
    def _():
        kforward(z)

    def silu_mul(g, u):
        return (g * (1.0 / (1.0 + jnp.exp(-g))) * u).astype(BF)

    def expert_part(k, side, shared):
        rows_in = gbuf[pl.ds(2 * k, 2)].reshape(2 * rows, width)
        g = jnp.dot(rows_in, gate[side], preferred_element_type=F32)
        u = jnp.dot(rows_in, up[side], preferred_element_type=F32)
        hidden = silu_mul(g, u)
        columns = []
        for s in range(2):
            turned = wbuf[2 * k + s].T
            lane = lax.broadcasted_iota(jnp.int32, turned.shape, 1)
            columns.append(jnp.sum(jnp.where(lane == z, turned, 0.0), axis=1, keepdims=True))
        weight = jnp.concatenate(columns, axis=0)
        half = width // 2
        for h in range(2):
            span = slice(h * half, (h + 1) * half)
            part = jnp.dot(hidden, down[side, :, span], preferred_element_type=F32) * weight
            part = part.reshape(2, rows, half)
            if side == 1:
                part = part + pbuf[k, :, :, span].astype(F32)
            pbuf[k, :, :, span] = part.astype(BF)

        @pl.when(shared)
        def _():
            if side == 1:
                for p in range(8, 11):
                    ycopy_in(p).wait_recv()
            sg = jnp.dot(rows_in, sgate[side], preferred_element_type=F32)
            su = jnp.dot(rows_in, sup[side], preferred_element_type=F32)
            sh = silu_mul(sg, su)
            for h in range(2):
                span = slice(h * half, (h + 1) * half)
                part = jnp.dot(sh, sdown[side, :, span], preferred_element_type=F32)
                before = pbuf[k, :, :, span].astype(F32)
                pbuf[k, :, :, span] = (before + part.reshape(2, rows, half)).astype(BF)

    def gather_step(j, carry):
        for jj, arriving in enumerate(((0, 1), (2, 3), (4, 5, 6, 7), (8, 9, 10))):

            @pl.when(j == jj)
            def _():
                for p in arriving:
                    xcopy(p).wait_recv()
                    ycopy(p).start()

        for i in range(1, 4):
            when = jnp.where(inner == 1, max(i - 2, 0), i - 1)

            @pl.when(j == when)
            def _():
                k = order(i)
                gwait_recv(2 * k + c)
                forward(k)
                if i == 3:

                    @pl.when(inner == 1)
                    def _():
                        kforward(z)

        k = order(j)
        gwait_recv(2 * k + 1 - c)
        expert_part(k, 0, j == 0)
        return carry

    lax.fori_loop(0, zn, gather_step, 0)

    def key_step(j, carry):
        k = order(j)
        kcopy(k, 0, partner_dev).wait_recv()
        kforward(k)
        return carry

    @pl.when(inner == 1)
    def _():
        lax.fori_loop(1, zn, key_step, 0)

    for p in range(8):
        ycopy_in(p).wait_recv()

    def ccopy(k, h, way, dev):
        span = pl.ds(h * (rows // 4), rows // 4)
        return remote(
            pbuf.at[k, c, span, :], cbuf.at[way, k, span, :], csend.at[k, h], crecv.at[way, k, h], dev
        )

    def pair_sum(k):
        acopy(k).wait_recv()
        for h in range(4):
            span = pl.ds(h * (rows // 4), rows // 4)
            pbuf[k, c, span, :] = (pbuf[k, c, span, :].astype(F32) + abuf[k, span, :].astype(F32)).astype(BF)

            @pl.when(jnp.logical_and(z == 0, k > z))
            def _():
                ccopy(k, h, 0, up_dev).start()

            @pl.when(jnp.logical_and(z == zn - 1, k < z))
            def _():
                ccopy(k, h, 1, dn_dev).start()

    def finish_step(i, carry):
        k = order(zn - 1 - i)
        expert_part(k, 1, i == zn - 1)
        acopy(k).start()

        @pl.when(i > 0)
        def _():
            pair_sum(order(zn - i))

        return carry

    lax.fori_loop(0, zn, finish_step, 0)
    pair_sum(z)

    @pl.when(inner == 0)
    def _():
        lax.fori_loop(1, zn, key_step, 0)

    heads = vw // hgain_ref.shape[1]
    head = kw // heads
    vdim = vw // heads
    qrows = arow // 3

    def attend_step(i, carry):
        r = pl.multiple_of(i * qrows, qrows)
        for h in range(heads):
            lane = lax.broadcasted_iota(jnp.int32, (qrows, kw), 1)
            mine = jnp.logical_and(lane >= h * head, lane < (h + 1) * head)
            outs = []
            for m, q_ref in enumerate((qa_ref, qb_ref)):
                q = jnp.where(mine, q_ref[pl.ds(r, qrows), :], jnp.zeros((), BF))
                keys = kbuf[:, :, m * kw : (m + 1) * kw].reshape(zn * arow, kw)
                s = lax.dot_general(q, keys, (((1,), (1,)), ((), ())), preferred_element_type=F32)
                s = s * (head ** -0.5)
                peak = jnp.max(s, axis=-1, keepdims=True)
                e = jnp.exp(s - peak)
                total = jnp.sum(e, axis=-1, keepdims=True)
                vals = kbuf[:, :, 2 * kw + h * vdim : 2 * kw + (h + 1) * vdim].reshape(zn * arow, vdim)
                o = jnp.dot(e.astype(BF), vals, preferred_element_type=F32)
                outs.append(o / total)
            mix = outs[0] - lam_ref[0, h] * outs[1]
            norm = lax.rsqrt(jnp.mean(mix * mix, axis=-1, keepdims=True) + epsilon)
            hout[pl.ds(r, qrows), h * vdim : (h + 1) * vdim] = (mix * norm * hgain_ref[...]).astype(BF)
        return carry


    orow = arow // tn

    def hcopy(to):
        return remote(
            hout.at[pl.ds(pl.multiple_of(to * orow, 16), orow), :],
            hbuf.at[t],
            hsend.at[to],
            hrecv.at[t],
            (grp, z, to),
        )

    def hrecv_wait(src):
        remote(
            hout.at[pl.ds(0, orow), :], hbuf.at[src], hsend.at[src], hrecv.at[src], (grp, z, src)
        ).wait_recv()

    def line_step(i, carry):
        k = order(jnp.where(i == 0, zn - 1, i))
        for h in range(4):
            span = pl.ds(h * (rows // 4), rows // 4)

            @pl.when(jnp.logical_and(k > z, has_dn))
            def _():
                ccopy(k, h, 0, up_dev).wait_recv()
                pbuf[k, c, span, :] = (
                    pbuf[k, c, span, :].astype(F32) + cbuf[0, k, span, :].astype(F32)
                ).astype(BF)
                ccopy(k, h, 0, up_dev).start()

            @pl.when(jnp.logical_and(k < z, has_up))
            def _():
                ccopy(k, h, 1, dn_dev).wait_recv()
                pbuf[k, c, span, :] = (
                    pbuf[k, c, span, :].astype(F32) + cbuf[1, k, span, :].astype(F32)
                ).astype(BF)
                ccopy(k, h, 1, dn_dev).start()

        lax.fori_loop(jnp.where(i == 0, 0, 1), jnp.where(i == 0, 1, jnp.where(i == 1, 3, 1)), attend_step, 0)

        @pl.when(i == 1)
        def _():
            for other in (peer, diag, partner):
                hcopy(other).start()
            hbuf[t] = hout[pl.ds(pl.multiple_of(t * orow, 16), orow), :]

        return carry

    lax.fori_loop(0, zn - 1, line_step, 0)

    for other in (partner, peer, diag):
        hrecv_wait(other)
    loads[9].wait()
    half = width // 2
    for h in range(2):
        acc = jnp.zeros((orow, half), F32)
        for s in range(tn):
            acc = acc + jnp.dot(
                hbuf[s], wo[s * vw : (s + 1) * vw, h * half : (h + 1) * half], preferred_element_type=F32
            )
        mixed_ref[:, h * half : (h + 1) * half] = acc.astype(BF)

    for h in range(4):
        span = pl.ds(h * (rows // 4), rows // 4)

        @pl.when(has_dn)
        def _():
            ccopy(z, h, 0, up_dev).wait_recv()
            pbuf[z, c, span, :] = (
                pbuf[z, c, span, :].astype(F32) + cbuf[0, z, span, :].astype(F32)
            ).astype(BF)

        @pl.when(has_up)
        def _():
            ccopy(z, h, 1, dn_dev).wait_recv()
            pbuf[z, c, span, :] = (
                pbuf[z, c, span, :].astype(F32) + cbuf[1, z, span, :].astype(F32)
            ).astype(BF)

    out_ref[...] = pbuf[z, c]

    def drain_step(k, carry):
        slot = 2 * k + c

        @pl.when(goes_up(k))
        def _():
            gwait_send(slot, 0, up_dev)
            kcopy(k, 0, up_dev).wait_send()

        @pl.when(goes_down(k))
        def _():
            gwait_send(slot, 1, dn_dev)
            kcopy(k, 1, dn_dev).wait_send()

        gwait_send(slot, 2, partner_dev)
        acopy(k).wait_send()

        @pl.when(k != z)
        def _():
            for h in range(4):
                ccopy(k, h, 0, up_dev).wait_send()

        return carry

    for p in range(len(pieces)):
        xcopy(p).wait_send()
        ycopy(p).wait_send()
    lax.fori_loop(0, zn, drain_step, 0)
    for other in (partner, peer, diag):
        hcopy(other).wait_send()


def fused_shards(
    zn,
    query_first,
    query_second,
    key_first,
    key_second,
    values,
    lambda_head,
    head_gain,
    out_weight,
    tokens,
    norm_gain,
    expert_ids,
    expert_weights,
    expert_gate,
    expert_up,
    expert_down,
    shared_gate,
    shared_up,
    shared_down,
):
    rows, width = tokens.shape
    arow, kw = key_first.shape
    vw = values.shape[1]
    tn = lax.axis_size("tp")
    pad = 8
    names = jnp.arange(pad, dtype=jnp.int32)[:, None]
    wloc = jnp.zeros((pad, rows), F32)
    for top in range(expert_ids.shape[1]):
        wloc = wloc + jnp.where(expert_ids[:, top][None, :] == names, expert_weights[:, top][None, :], 0.0)
    vmem = pl.BlockSpec(memory_space=pltpu.VMEM)
    smem = pl.BlockSpec(memory_space=pltpu.SMEM)
    hbm = pl.BlockSpec(memory_space=pltpu.HBM)
    dma = pltpu.SemaphoreType.DMA
    slots = zn * 2
    hidden = expert_gate.shape[2]
    shared = shared_gate.shape[1]
    mixed, expert_out = pl.pallas_call(
        functools.partial(fused_kernel, zn),
        out_shape=(
            jax.ShapeDtypeStruct((arow // tn, width), BF),
            jax.ShapeDtypeStruct((rows, width), BF),
        ),
        in_specs=[vmem, vmem, vmem, vmem, vmem, hbm, hbm, hbm, smem, vmem] + [hbm] * 7,
        out_specs=(vmem, vmem),
        scratch_shapes=[
            pltpu.VMEM((slots, rows, width), BF),
            pltpu.VMEM((slots, pad, rows), F32),
            pltpu.VMEM((zn, arow, 2 * kw + vw), BF),
            pltpu.VMEM((zn, 2, rows, width), BF),
            pltpu.VMEM((zn, rows, width), BF),
            pltpu.VMEM((2, zn, rows, width), BF),
            pltpu.VMEM((arow, vw), BF),
            pltpu.VMEM((tn, arow // tn, vw), BF),
            pltpu.VMEM((2, width, hidden), BF),
            pltpu.VMEM((2, width, hidden), BF),
            pltpu.VMEM((2, hidden, width), BF),
            pltpu.VMEM((2, width, shared), BF),
            pltpu.VMEM((2, width, shared), BF),
            pltpu.VMEM((2, shared, width), BF),
            pltpu.VMEM(out_weight.shape, BF),
            dma((10,)),
            dma((3, slots)),
            dma((slots,)),
            dma((3, slots)),
            dma((slots,)),
            dma((2, zn)),
            dma((zn,)),
            dma((zn,)),
            dma((zn,)),
            dma((11,)),
            dma((11,)),
            dma((11,)),
            dma((11,)),
            dma((zn, 4)),
            dma((2, zn, 4)),
            dma((tn,)),
            dma((tn,)),
        ],
        compiler_params=pltpu.CompilerParams(
            collective_id=0, has_side_effects=True, vmem_limit_bytes=66000000
        ),
    )(
        tokens,
        norm_gain[None, :],
        wloc,
        query_first,
        query_second,
        key_first,
        key_second,
        values,
        lambda_head[None, :],
        head_gain[None, :],
        expert_gate,
        expert_up,
        expert_down,
        shared_gate,
        shared_up,
        shared_down,
        out_weight,
    )
    return mixed, expert_out


def solution(mesh):
    placed = (
        P(("grp", "ep"), "tp"),
        P(("grp", "ep"), "tp"),
        P(("grp", "ep"), "tp"),
        P(("grp", "ep"), "tp"),
        P(("grp", "ep"), "tp"),
        P("tp"),
        P(),
        P(),
        P(("grp", "ep", "tp"), None),
        P(),
        P(("grp", "ep", "tp"), None),
        P(("grp", "ep", "tp"), None),
        P("ep", None, "tp"),
        P("ep", None, "tp"),
        P("ep", "tp", None),
        P(None, "tp"),
        P(None, "tp"),
        P("tp", None),
    )
    body = functools.partial(fused_shards, mesh.shape["ep"]) if fused_fits(mesh) else shards
    return jax.shard_map(
        body,
        mesh=mesh,
        in_specs=placed,
        out_specs=(P(("grp", "ep", "tp"), None), P(("grp", "ep", "tp"), None)),
        check_vma=False,
    )
```

```python
import jax
import jax.numpy as jnp
from jax import lax
from jax.experimental import pallas as pl
from jax.experimental.pallas import tpu as pltpu
import functools
from jax.sharding import PartitionSpec as P

epsilon = 1e-06
block_limit = 1536


def key_block(total_rows, shard_rows):
    if total_rows <= block_limit or total_rows % shard_rows != 0:
        return total_rows
    best_rows = shard_rows
    for factor_rows in range(1, total_rows // shard_rows + 1):
        if total_rows % (factor_rows * shard_rows) == 0 and factor_rows * shard_rows <= block_limit:
            best_rows = factor_rows * shard_rows
    return best_rows


def softmax_update(states, scores, value_block):
    running_max, running_sum, accumulated = states
    new_max = jnp.maximum(running_max, jnp.max(scores, axis=-1))
    rescale = jnp.exp(running_max - new_max)
    weights = jnp.exp(scores - new_max[..., None])
    new_sum = running_sum * rescale + jnp.sum(weights, axis=-1)
    product = jnp.einsum(
        "qhk,khe->qhe",
        weights.astype(jnp.bfloat16),
        value_block,
        preferred_element_type=jnp.float32,
    )
    return (new_max, new_sum, accumulated * rescale[..., None] + product)


def shards(
    query_first,
    query_second,
    key_first,
    key_second,
    values,
    lambda_head,
    head_gain,
    out_weight,
    tokens,
    norm_gain,
    expert_ids,
    expert_weights,
    expert_gate,
    expert_up,
    expert_down,
    shared_gate,
    shared_up,
    shared_down,
):
    shard_rows, query_width = query_first.shape
    heads_here = lambda_head.shape[0]
    head_size = query_width // heads_here
    value_size = values.shape[1] // heads_here
    score_scale = head_size ** (-0.5)
    query_one = query_first.reshape(shard_rows, heads_here, head_size)
    query_two = query_second.reshape(shard_rows, heads_here, head_size)
    initial = (
        jnp.full((shard_rows, heads_here), -jnp.inf, jnp.float32),
        jnp.zeros((shard_rows, heads_here), jnp.float32),
        jnp.zeros((shard_rows, heads_here, value_size), jnp.float32),
    )
    carried = (initial, initial)
    key_one = lax.all_gather(key_first, "ep", axis=0, tiled=True)
    key_two = lax.all_gather(key_second, "ep", axis=0, tiled=True)
    value_piece = lax.all_gather(values, "ep", axis=0, tiled=True)
    total_rows = key_one.shape[0]
    block_rows = key_block(total_rows, shard_rows)
    block_count = total_rows // block_rows
    stacked = (
        key_one.reshape(block_count, block_rows, heads_here, head_size),
        key_two.reshape(block_count, block_rows, heads_here, head_size),
        value_piece.reshape(block_count, block_rows, heads_here, value_size),
    )

    def fold_step(states, blocks):
        first_state, second_state = states
        key_a, key_b, value_block = blocks
        scores_a = (
            jnp.einsum("qhd,khd->qhk", query_one, key_a, preferred_element_type=jnp.float32)
            * score_scale
        )
        scores_b = (
            jnp.einsum("qhd,khd->qhk", query_two, key_b, preferred_element_type=jnp.float32)
            * score_scale
        )
        return (
            (
                softmax_update(first_state, scores_a, value_block),
                softmax_update(second_state, scores_b, value_block),
            ),
            None,
        )

    carried, unused = lax.scan(fold_step, carried, stacked)
    first_state, second_state = carried
    first_out = first_state[2] / first_state[1][..., None]
    second_out = second_state[2] / second_state[1][..., None]
    mixture = first_out - lambda_head[None, :, None] * second_out
    normed_heads = (
        mixture
        * lax.rsqrt(jnp.mean(mixture * mixture, axis=-1, keepdims=True) + epsilon)
        * head_gain
    )
    head_local = normed_heads.astype(jnp.bfloat16).reshape(shard_rows, heads_here * value_size)
    position_heads = lax.all_to_all(head_local, "tp", split_axis=0, concat_axis=1, tiled=True)
    mixed = jnp.dot(position_heads, out_weight, preferred_element_type=jnp.float32).astype(
        jnp.bfloat16
    )
    row_count, model_width = tokens.shape
    top_count = expert_ids.shape[1]
    ep_count = lax.axis_size("ep")
    local_experts = expert_gate.shape[0]
    expert_count = local_experts * ep_count
    capacity = max(2, row_count * top_count * 3 // (2 * expert_count))
    routed_rows = expert_count * capacity
    owner_span = routed_rows + row_count
    widened = tokens.astype(jnp.float32)
    normed = (
        widened
        * lax.rsqrt(jnp.mean(widened * widened, axis=-1, keepdims=True) + epsilon)
        * norm_gain
    ).astype(jnp.bfloat16)
    flat_ids = expert_ids.reshape(-1)
    onehot = (flat_ids[:, None] == jnp.arange(expert_count, dtype=jnp.int32)[None, :]).astype(
        jnp.int32
    )
    ranks = jnp.sum(onehot * jnp.cumsum(onehot, axis=0), axis=1) - 1
    slot_index = flat_ids * capacity + ranks
    token_index = jnp.arange(flat_ids.shape[0], dtype=jnp.int32) // top_count
    filled = jnp.full((routed_rows,), row_count, jnp.int32).at[slot_index].set(token_index)
    padded = jnp.concatenate([normed, jnp.zeros((1, model_width), jnp.bfloat16)], axis=0)
    outgoing = padded[filled].reshape(1, ep_count, local_experts * capacity, model_width)
    arrived = lax.all_to_all(outgoing, "ep", split_axis=1, concat_axis=1, tiled=True)
    local_rows = jnp.concatenate(
        [arrived.reshape(1, routed_rows, model_width), normed[None]], axis=1
    )
    gathered = lax.all_gather(local_rows, "tp", axis=0, tiled=True)
    owners = owner_span * lax.axis_size("tp") // owner_span
    routed_in = gathered[:, :routed_rows].reshape(
        owners, ep_count, local_experts, capacity, model_width
    )
    gate_value = jnp.einsum(
        "osecd,edf->osecf", routed_in, expert_gate, preferred_element_type=jnp.float32
    )
    up_value = jnp.einsum(
        "osecd,edf->osecf", routed_in, expert_up, preferred_element_type=jnp.float32
    )
    hidden = (jax.nn.silu(gate_value) * up_value).astype(jnp.bfloat16)
    routed_out = jnp.einsum(
        "osecf,efd->osecd", hidden, expert_down, preferred_element_type=jnp.float32
    )
    routed_out = routed_out.reshape(owners, routed_rows, model_width)
    shared_in = gathered[:, routed_rows:]
    shared_gate_value = jnp.einsum(
        "ord,df->orf", shared_in, shared_gate, preferred_element_type=jnp.float32
    )
    shared_up_value = jnp.einsum(
        "ord,df->orf", shared_in, shared_up, preferred_element_type=jnp.float32
    )
    shared_hidden = (jax.nn.silu(shared_gate_value) * shared_up_value).astype(jnp.bfloat16)
    shared_out = jnp.einsum(
        "orf,fd->ord", shared_hidden, shared_down, preferred_element_type=jnp.float32
    )
    kept_rows = lax.psum_scatter(
        jnp.concatenate([routed_out, shared_out], axis=1)
        .reshape(owners * owner_span, model_width)
        .astype(jnp.bfloat16),
        "tp",
        scatter_dimension=0,
        tiled=True,
    ).astype(jnp.float32)
    routed_back = (
        kept_rows[:routed_rows]
        .astype(jnp.bfloat16)
        .reshape(ep_count, local_experts * capacity, model_width)
    )
    returned = lax.all_to_all(routed_back, "ep", split_axis=0, concat_axis=0, tiled=True).reshape(
        routed_rows, model_width
    )
    picked = returned[slot_index].reshape(row_count, top_count, model_width).astype(jnp.float32)
    combined = jnp.sum(picked * expert_weights[:, :, None], axis=1) + kept_rows[routed_rows:]
    expert_out = combined.astype(jnp.bfloat16)
    return (mixed, expert_out)


MESH = pl.DeviceIdType.MESH
BF = jnp.bfloat16
F32 = jnp.float32


def fused_fits(mesh):
    return mesh.shape["grp"] == 2 and mesh.shape["ep"] == 4 and mesh.shape["tp"] == 4


def fused_kernel(
    zn,
    tokens_ref,
    gain_ref,
    wloc_ref,
    qa_ref,
    qb_ref,
    ka_hbm,
    kb_hbm,
    v_hbm,
    lam_ref,
    hgain_ref,
    gate_hbm,
    up_hbm,
    down_hbm,
    sgate_hbm,
    sup_hbm,
    sdown_hbm,
    wo_hbm,
    mixed_ref,
    out_ref,
    gbuf,
    wbuf,
    kbuf,
    pbuf,
    abuf,
    cbuf,
    hout,
    hbuf,
    gate,
    up,
    down,
    sgate,
    sup,
    sdown,
    wo,
    lsem,
    gsend,
    grecv,
    wsend,
    wrecv,
    ksend,
    krecv,
    asend,
    arecv,
    xsend,
    xrecv,
    ysend,
    yrecv,
    csend,
    crecv,
    hsend,
    hrecv,
):
    grp = lax.axis_index("grp")
    z = lax.axis_index("ep")
    t = lax.axis_index("tp")
    c = lax.rem(t, 2)
    x = lax.div(t, 2)
    partner = 2 * x + 1 - c
    peer = 2 * (1 - x) + c
    diag = 2 * (1 - x) + 1 - c
    tn = 4
    rows = tokens_ref.shape[0]
    width = tokens_ref.shape[1]
    arow = qa_ref.shape[0]
    kw = ka_hbm.shape[1]
    vw = v_hbm.shape[1]

    has_up = z < zn - 1
    has_dn = z > 0
    up_dev = (grp, jnp.minimum(z + 1, zn - 1), t)
    dn_dev = (grp, jnp.maximum(z - 1, 0), t)
    partner_dev = (grp, z, partner)
    peer_dev = (grp, z, peer)
    twin_dev = (1 - grp, z, t)

    loads = [
        pltpu.make_async_copy(ka_hbm, kbuf.at[z, :, pl.ds(0, kw)], lsem.at[0]),
        pltpu.make_async_copy(kb_hbm, kbuf.at[z, :, pl.ds(kw, kw)], lsem.at[1]),
        pltpu.make_async_copy(v_hbm, kbuf.at[z, :, pl.ds(2 * kw, vw)], lsem.at[2]),
        pltpu.make_async_copy(gate_hbm.at[0], gate.at[0], lsem.at[3]),
        pltpu.make_async_copy(up_hbm.at[0], up.at[0], lsem.at[4]),
        pltpu.make_async_copy(down_hbm.at[0], down.at[0], lsem.at[5]),
        pltpu.make_async_copy(sgate_hbm, sgate.at[0], lsem.at[6]),
        pltpu.make_async_copy(sup_hbm, sup.at[0], lsem.at[7]),
        pltpu.make_async_copy(sdown_hbm, sdown.at[0], lsem.at[8]),
        pltpu.make_async_copy(wo_hbm, wo, lsem.at[9]),
    ]
    for load in loads[3:] + loads[:3]:
        load.start()

    barrier = pltpu.get_barrier_semaphore()
    for other in (partner, peer, diag):
        pl.semaphore_signal(barrier, inc=1, device_id=(grp, z, other), device_id_type=MESH)
    pl.semaphore_signal(barrier, inc=1, device_id=twin_dev, device_id_type=MESH)

    @pl.when(has_up)
    def _():
        pl.semaphore_signal(barrier, inc=1, device_id=up_dev, device_id_type=MESH)

    @pl.when(has_dn)
    def _():
        pl.semaphore_signal(barrier, inc=1, device_id=dn_dev, device_id_type=MESH)

    own = 2 * z + c
    wide = tokens_ref[...].astype(F32)
    scale = lax.rsqrt(jnp.mean(wide * wide, axis=-1, keepdims=True) + epsilon)
    gbuf[own] = (wide * scale * gain_ref[...]).astype(BF)
    wbuf[own] = wloc_ref[...]

    pl.semaphore_wait(barrier, 4 + jnp.where(has_up, 1, 0) + jnp.where(has_dn, 1, 0))

    def remote(src, dst, ssem, rsem, dev):
        return pltpu.make_async_remote_copy(
            src_ref=src, dst_ref=dst, send_sem=ssem, recv_sem=rsem, device_id=dev, device_id_type=MESH
        )

    def gcopies(slot, way, dev):
        return (
            remote(gbuf.at[slot], gbuf.at[slot], gsend.at[way, slot], grecv.at[slot], dev),
            remote(wbuf.at[slot], wbuf.at[slot], wsend.at[way, slot], wrecv.at[slot], dev),
        )

    def gstart(slot, way, dev):
        for one in gcopies(slot, way, dev):
            one.start()

    def gwait_recv(slot):
        for one in gcopies(slot, 0, partner_dev):
            one.wait_recv()

    def gwait_send(slot, way, dev):
        for one in gcopies(slot, way, dev):
            one.wait_send()

    def goes_up(k):
        return jnp.logical_and(has_up, k <= z)

    def goes_down(k):
        return jnp.logical_and(has_dn, k >= z)

    def order(j):
        low = jnp.minimum(z, zn - 1 - z)
        first = jnp.where(j < 2, 1 - j, j)
        near = jnp.where(low == 1, first, j)
        return jnp.where(z < 2, near, zn - 1 - near)

    def forward(k):
        slot = 2 * k + c

        @pl.when(goes_up(k))
        def _():
            gstart(slot, 0, up_dev)

        @pl.when(goes_down(k))
        def _():
            gstart(slot, 1, dn_dev)

        gstart(slot, 2, partner_dev)

    forward(z)
    inner = jnp.minimum(z, zn - 1 - z)

    def kcopy(k, way, dev):
        return remote(kbuf.at[k], kbuf.at[k], ksend.at[way, k], krecv.at[k], dev)

    def kforward(k):
        @pl.when(goes_up(k))
        def _():
            kcopy(k, 0, up_dev).start()

        @pl.when(goes_down(k))
        def _():
            kcopy(k, 1, dn_dev).start()

    def acopy(k):
        return remote(pbuf.at[k, 1 - c], abuf.at[k], asend.at[k], arecv.at[k], partner_dev)

    def cuts(buf, parts):
        size = buf.shape[1] // (2 * parts)
        return [(buf, (grp * parts + q) * size, (parts - grp * parts + q) * size, size) for q in range(parts)]

    pieces = cuts(gate, 2) + cuts(up, 2) + cuts(down, 4) + cuts(sgate, 1) + cuts(sup, 1) + cuts(sdown, 1)

    def xcopy(p):
        buf, mine, _, size = pieces[p]
        span = pl.ds(pl.multiple_of(mine, 16), size)
        return remote(buf.at[0, span, :], buf.at[1, span, :], xsend.at[p], xrecv.at[p], peer_dev)

    def ycopy(p):
        buf, mine, _, size = pieces[p]
        span = pl.ds(pl.multiple_of(mine, 16), size)
        return remote(buf.at[1, span, :], buf.at[1, span, :], ysend.at[p], yrecv.at[p], twin_dev)

    def ycopy_in(p):
        buf, _, theirs, size = pieces[p]
        span = pl.ds(pl.multiple_of(theirs, 16), size)
        return remote(buf.at[1, span, :], buf.at[1, span, :], ysend.at[p], yrecv.at[p], twin_dev)

    for p in range(len(pieces)):
        if p in (0, 2, 4):
            loads[3 + p // 2].wait()
        if p >= 8:
            loads[p - 2].wait()
        xcopy(p).start()
    for load in loads[:3]:
        load.wait()

    @pl.when(inner == 0)
    def _():
        kforward(z)

    def silu_mul(g, u):
        return (g * (1.0 / (1.0 + jnp.exp(-g))) * u).astype(BF)

    def expert_part(k, side, shared):
        rows_in = gbuf[pl.ds(2 * k, 2)].reshape(2 * rows, width)
        g = jnp.dot(rows_in, gate[side], preferred_element_type=F32)
        u = jnp.dot(rows_in, up[side], preferred_element_type=F32)
        hidden = silu_mul(g, u)
        columns = []
        for s in range(2):
            turned = wbuf[2 * k + s].T
            lane = lax.broadcasted_iota(jnp.int32, turned.shape, 1)
            columns.append(jnp.sum(jnp.where(lane == z, turned, 0.0), axis=1, keepdims=True))
        weight = jnp.concatenate(columns, axis=0)
        half = width // 2
        for h in range(2):
            span = slice(h * half, (h + 1) * half)
            part = jnp.dot(hidden, down[side, :, span], preferred_element_type=F32) * weight
            part = part.reshape(2, rows, half)
            if side == 1:
                part = part + pbuf[k, :, :, span].astype(F32)
            pbuf[k, :, :, span] = part.astype(BF)

        @pl.when(shared)
        def _():
            if side == 1:
                for p in range(8, 11):
                    ycopy_in(p).wait_recv()
            sg = jnp.dot(rows_in, sgate[side], preferred_element_type=F32)
            su = jnp.dot(rows_in, sup[side], preferred_element_type=F32)
            sh = silu_mul(sg, su)
            for h in range(2):
                span = slice(h * half, (h + 1) * half)
                part = jnp.dot(sh, sdown[side, :, span], preferred_element_type=F32)
                before = pbuf[k, :, :, span].astype(F32)
                pbuf[k, :, :, span] = (before + part.reshape(2, rows, half)).astype(BF)

    def gather_step(j, carry):
        for jj, arriving in enumerate(((0, 1), (2, 3), (4, 5, 6, 7))):

            @pl.when(j == jj)
            def _():
                for p in arriving:
                    xcopy(p).wait_recv()
                    ycopy(p).start()

        for i in range(1, 4):
            when = jnp.where(inner == 1, max(i - 2, 0), i - 1)

            @pl.when(j == when)
            def _():
                k = order(i)
                gwait_recv(2 * k + c)
                forward(k)
                if i == 3:

                    @pl.when(inner == 1)
                    def _():
                        kforward(z)

        k = order(j)
        gwait_recv(2 * k + 1 - c)
        expert_part(k, 0, j == 0)
        return carry

    lax.fori_loop(0, zn, gather_step, 0)

    def key_step(j, carry):
        k = order(j)
        kcopy(k, 0, partner_dev).wait_recv()
        kforward(k)
        return carry

    @pl.when(inner == 1)
    def _():
        lax.fori_loop(1, zn, key_step, 0)

    for p in range(8):
        ycopy_in(p).wait_recv()

    def ccopy(k, h, way, dev):
        span = pl.ds(h * (rows // 4), rows // 4)
        return remote(
            pbuf.at[k, c, span, :], cbuf.at[way, k, span, :], csend.at[k, h], crecv.at[way, k, h], dev
        )

    def pair_sum(k):
        acopy(k).wait_recv()
        for h in range(4):
            span = pl.ds(h * (rows // 4), rows // 4)
            pbuf[k, c, span, :] = (pbuf[k, c, span, :].astype(F32) + abuf[k, span, :].astype(F32)).astype(BF)

            @pl.when(jnp.logical_and(z == 0, k > z))
            def _():
                ccopy(k, h, 0, up_dev).start()

            @pl.when(jnp.logical_and(z == zn - 1, k < z))
            def _():
                ccopy(k, h, 1, dn_dev).start()

    def finish_step(i, carry):
        k = order(zn - 1 - i)

        @pl.when(i == zn - 2)
        def _():
            for p in range(8, 11):
                xcopy(p).wait_recv()
                ycopy(p).start()

        expert_part(k, 1, i == zn - 1)
        acopy(k).start()

        @pl.when(i > 0)
        def _():
            pair_sum(order(zn - i))

        return carry

    lax.fori_loop(0, zn, finish_step, 0)
    pair_sum(z)

    @pl.when(inner == 0)
    def _():
        lax.fori_loop(1, zn, key_step, 0)

    heads = vw // hgain_ref.shape[1]
    head = kw // heads
    vdim = vw // heads
    qrows = arow // 3

    def attend_step(i, carry):
        r = pl.multiple_of(i * qrows, qrows)
        for h in range(heads):
            lane = lax.broadcasted_iota(jnp.int32, (qrows, kw), 1)
            mine = jnp.logical_and(lane >= h * head, lane < (h + 1) * head)
            outs = []
            for m, q_ref in enumerate((qa_ref, qb_ref)):
                q = jnp.where(mine, q_ref[pl.ds(r, qrows), :], jnp.zeros((), BF))
                keys = kbuf[:, :, m * kw : (m + 1) * kw].reshape(zn * arow, kw)
                s = lax.dot_general(q, keys, (((1,), (1,)), ((), ())), preferred_element_type=F32)
                s = s * (head ** -0.5)
                peak = jnp.max(s, axis=-1, keepdims=True)
                e = jnp.exp(s - peak)
                total = jnp.sum(e, axis=-1, keepdims=True)
                vals = kbuf[:, :, 2 * kw + h * vdim : 2 * kw + (h + 1) * vdim].reshape(zn * arow, vdim)
                o = jnp.dot(e.astype(BF), vals, preferred_element_type=F32)
                outs.append(o / total)
            mix = outs[0] - lam_ref[0, h] * outs[1]
            norm = lax.rsqrt(jnp.mean(mix * mix, axis=-1, keepdims=True) + epsilon)
            hout[pl.ds(r, qrows), h * vdim : (h + 1) * vdim] = (mix * norm * hgain_ref[...]).astype(BF)
        return carry


    orow = arow // tn

    def hcopy(to):
        return remote(
            hout.at[pl.ds(pl.multiple_of(to * orow, 16), orow), :],
            hbuf.at[t],
            hsend.at[to],
            hrecv.at[t],
            (grp, z, to),
        )

    def hrecv_wait(src):
        remote(
            hout.at[pl.ds(0, orow), :], hbuf.at[src], hsend.at[src], hrecv.at[src], (grp, z, src)
        ).wait_recv()

    def line_step(i, carry):
        k = order(jnp.where(i == 0, zn - 1, i))
        for h in range(4):
            span = pl.ds(h * (rows // 4), rows // 4)

            @pl.when(jnp.logical_and(k > z, has_dn))
            def _():
                ccopy(k, h, 0, up_dev).wait_recv()
                pbuf[k, c, span, :] = (
                    pbuf[k, c, span, :].astype(F32) + cbuf[0, k, span, :].astype(F32)
                ).astype(BF)
                ccopy(k, h, 0, up_dev).start()

            @pl.when(jnp.logical_and(k < z, has_up))
            def _():
                ccopy(k, h, 1, dn_dev).wait_recv()
                pbuf[k, c, span, :] = (
                    pbuf[k, c, span, :].astype(F32) + cbuf[1, k, span, :].astype(F32)
                ).astype(BF)
                ccopy(k, h, 1, dn_dev).start()

        lax.fori_loop(jnp.where(i == 0, 0, 1), jnp.where(i == 0, 1, jnp.where(i == 1, 3, 1)), attend_step, 0)

        @pl.when(i == 1)
        def _():
            for other in (peer, diag, partner):
                hcopy(other).start()
            hbuf[t] = hout[pl.ds(pl.multiple_of(t * orow, 16), orow), :]

        return carry

    lax.fori_loop(0, zn - 1, line_step, 0)

    for other in (partner, peer, diag):
        hrecv_wait(other)
    loads[9].wait()
    half = width // 2
    for h in range(2):
        acc = jnp.zeros((orow, half), F32)
        for s in range(tn):
            acc = acc + jnp.dot(
                hbuf[s], wo[s * vw : (s + 1) * vw, h * half : (h + 1) * half], preferred_element_type=F32
            )
        mixed_ref[:, h * half : (h + 1) * half] = acc.astype(BF)

    for h in range(4):
        span = pl.ds(h * (rows // 4), rows // 4)

        @pl.when(has_dn)
        def _():
            ccopy(z, h, 0, up_dev).wait_recv()
            pbuf[z, c, span, :] = (
                pbuf[z, c, span, :].astype(F32) + cbuf[0, z, span, :].astype(F32)
            ).astype(BF)

        @pl.when(has_up)
        def _():
            ccopy(z, h, 1, dn_dev).wait_recv()
            pbuf[z, c, span, :] = (
                pbuf[z, c, span, :].astype(F32) + cbuf[1, z, span, :].astype(F32)
            ).astype(BF)

    out_ref[...] = pbuf[z, c]

    def drain_step(k, carry):
        slot = 2 * k + c

        @pl.when(goes_up(k))
        def _():
            gwait_send(slot, 0, up_dev)
            kcopy(k, 0, up_dev).wait_send()

        @pl.when(goes_down(k))
        def _():
            gwait_send(slot, 1, dn_dev)
            kcopy(k, 1, dn_dev).wait_send()

        gwait_send(slot, 2, partner_dev)
        acopy(k).wait_send()

        @pl.when(k != z)
        def _():
            for h in range(4):
                ccopy(k, h, 0, up_dev).wait_send()

        return carry

    for p in range(len(pieces)):
        xcopy(p).wait_send()
        ycopy(p).wait_send()
    lax.fori_loop(0, zn, drain_step, 0)
    for other in (partner, peer, diag):
        hcopy(other).wait_send()


def fused_shards(
    zn,
    query_first,
    query_second,
    key_first,
    key_second,
    values,
    lambda_head,
    head_gain,
    out_weight,
    tokens,
    norm_gain,
    expert_ids,
    expert_weights,
    expert_gate,
    expert_up,
    expert_down,
    shared_gate,
    shared_up,
    shared_down,
):
    rows, width = tokens.shape
    arow, kw = key_first.shape
    vw = values.shape[1]
    tn = lax.axis_size("tp")
    pad = 8
    names = jnp.arange(pad, dtype=jnp.int32)[:, None]
    wloc = jnp.zeros((pad, rows), F32)
    for top in range(expert_ids.shape[1]):
        wloc = wloc + jnp.where(expert_ids[:, top][None, :] == names, expert_weights[:, top][None, :], 0.0)
    vmem = pl.BlockSpec(memory_space=pltpu.VMEM)
    smem = pl.BlockSpec(memory_space=pltpu.SMEM)
    hbm = pl.BlockSpec(memory_space=pltpu.HBM)
    dma = pltpu.SemaphoreType.DMA
    slots = zn * 2
    hidden = expert_gate.shape[2]
    shared = shared_gate.shape[1]
    mixed, expert_out = pl.pallas_call(
        functools.partial(fused_kernel, zn),
        out_shape=(
            jax.ShapeDtypeStruct((arow // tn, width), BF),
            jax.ShapeDtypeStruct((rows, width), BF),
        ),
        in_specs=[vmem, vmem, vmem, vmem, vmem, hbm, hbm, hbm, smem, vmem] + [hbm] * 7,
        out_specs=(vmem, vmem),
        scratch_shapes=[
            pltpu.VMEM((slots, rows, width), BF),
            pltpu.VMEM((slots, pad, rows), F32),
            pltpu.VMEM((zn, arow, 2 * kw + vw), BF),
            pltpu.VMEM((zn, 2, rows, width), BF),
            pltpu.VMEM((zn, rows, width), BF),
            pltpu.VMEM((2, zn, rows, width), BF),
            pltpu.VMEM((arow, vw), BF),
            pltpu.VMEM((tn, arow // tn, vw), BF),
            pltpu.VMEM((2, width, hidden), BF),
            pltpu.VMEM((2, width, hidden), BF),
            pltpu.VMEM((2, hidden, width), BF),
            pltpu.VMEM((2, width, shared), BF),
            pltpu.VMEM((2, width, shared), BF),
            pltpu.VMEM((2, shared, width), BF),
            pltpu.VMEM(out_weight.shape, BF),
            dma((10,)),
            dma((3, slots)),
            dma((slots,)),
            dma((3, slots)),
            dma((slots,)),
            dma((2, zn)),
            dma((zn,)),
            dma((zn,)),
            dma((zn,)),
            dma((11,)),
            dma((11,)),
            dma((11,)),
            dma((11,)),
            dma((zn, 4)),
            dma((2, zn, 4)),
            dma((tn,)),
            dma((tn,)),
        ],
        compiler_params=pltpu.CompilerParams(
            collective_id=0, has_side_effects=True, vmem_limit_bytes=66000000
        ),
    )(
        tokens,
        norm_gain[None, :],
        wloc,
        query_first,
        query_second,
        key_first,
        key_second,
        values,
        lambda_head[None, :],
        head_gain[None, :],
        expert_gate,
        expert_up,
        expert_down,
        shared_gate,
        shared_up,
        shared_down,
        out_weight,
    )
    return mixed, expert_out


def solution(mesh):
    placed = (
        P(("grp", "ep"), "tp"),
        P(("grp", "ep"), "tp"),
        P(("grp", "ep"), "tp"),
        P(("grp", "ep"), "tp"),
        P(("grp", "ep"), "tp"),
        P("tp"),
        P(),
        P(),
        P(("grp", "ep", "tp"), None),
        P(),
        P(("grp", "ep", "tp"), None),
        P(("grp", "ep", "tp"), None),
        P("ep", None, "tp"),
        P("ep", None, "tp"),
        P("ep", "tp", None),
        P(None, "tp"),
        P(None, "tp"),
        P("tp", None),
    )
    body = functools.partial(fused_shards, mesh.shape["ep"]) if fused_fits(mesh) else shards
    return jax.shard_map(
        body,
        mesh=mesh,
        in_specs=placed,
        out_specs=(P(("grp", "ep", "tp"), None), P(("grp", "ep", "tp"), None)),
        check_vma=False,
    )
```
